256 devices in a mesh: ep: 64 (over z, x, core), tp: 4 (over y).
Axes of the slice: x: 4, y: 4, z: 8, core: 2. Of those that a mesh axis runs over, the one named last changes fastest.
Arguments:
- tokens: bfloat16 [1024, 2048], P('ep'), may hold values from -6 to 6
- attn_gain: float32 [2048], replicated, may hold values from 0.1 to 1.9
- query_weight: bfloat16 [2048, 2048], P('ep', 'tp'), may hold values from -0.125 to 0.125
- key_weight: bfloat16 [2048, 512], P('ep', 'tp'), may hold values from -0.125 to 0.125
- value_weight: bfloat16 [2048, 512], P('ep', 'tp'), may hold values from -0.125 to 0.125
- break_bias: float32 [16], P('tp'), may hold values from -14 to -8
- cache_keys: bfloat16 [1024, 4, 1024, 128], P('ep', 'tp'), may hold values from -18 to 18
- cache_values: bfloat16 [1024, 4, 1024, 128], P('ep', 'tp'), may hold values from -6 to 6
- lengths: int32 [1024], P('ep'), may hold values from 1 to 1024, 524288 in all
- out_weight: bfloat16 [2048, 2048], P('tp', 'ep'), may hold values from -0.25 to 0.25
- ffn_gain: float32 [2048], replicated, may hold values from 0.1 to 1.9
- branch_gate: bfloat16 [2048], replicated, may hold values from -0.125 to 0.125
- dense_gate: bfloat16 [2048, 8192], P('tp', 'ep'), may hold values from -0.125 to 0.125
- dense_up: bfloat16 [2048, 8192], P('tp', 'ep'), may hold values from -0.125 to 0.125
- dense_down: bfloat16 [8192, 2048], P('ep', 'tp'), may hold values from -0.0625 to 0.0625
- route_ids: int32 [1024, 4], P('ep'), may hold values from 0 to 63, all different within a row; in each aligned block of 16 rows (0 to 15, 16 to 31, ...) at most 2 rows name the same one
- route_weights: float32 [1024, 4], P('ep'), may hold values from 0.1 to 1
- expert_gate: bfloat16 [64, 2048, 1024], P('ep', None, 'tp'), may hold values from -0.4375 to 0.4375
- expert_up: bfloat16 [64, 2048, 1024], P('ep', None, 'tp'), may hold values from -0.4375 to 0.4375
- expert_down: bfloat16 [64, 1024, 2048], P('ep', 'tp'), may hold values from -0.01953125 to 0.01953125
Outputs:
- layer_out: bfloat16 [1024, 2048], P('ep', 'tp')
- new_keys: bfloat16 [1024, 512], P('ep', 'tp')
- new_values: bfloat16 [1024, 512], P('ep', 'tp')
The draws below stay inside these ranges and needn't reach their ends.
Inputs may be any that keep to these rules, and one draw needn't show every extreme that they name: `route_ids`: each row names 4 different experts. Among the rows of one device no expert is named more than 2 times, a bound that some block reaches. Sequence b's cache holds keys at positions below lengths[b]; some sequence fills its whole cache.
All inputs are finite; a program needn't handle non-finite values. No bound on the sum of `lengths` on one device may be relied on, other than what follows from the above.
Results may differ from the reference program's by a relative error of at most 0.011.
Values may be sent and summed in bfloat16 or wider, within the bound.
A program may use at most 64 MiB of HBM per device.

```python
import math
import jax
import jax.numpy as jnp
import numpy as np
from jax import lax

D = 2048
HEADS = 16
KV_HEADS = 4
HEAD_DIM = 128
DENSE = 8192
EXPERT_W = 1024
TOP_K = 4
SEQS = 16
CACHE_LEN = 1024
SEQUENCES = 1024
EXPERTS = 64
CAP = 2
N_EP = 64


def levels(key, extent, split, smallest, high):
    def one(axis_at, shards_of):
        draws = jax.random.uniform(jax.random.fold_in(jax.random.fold_in(key, 6), axis_at), (shards_of,), jnp.float32, smallest / len(split), high / len(split))
        return jnp.repeat(jnp.exp(draws), extent[axis_at] // shards_of).reshape((-1,) + (1,) * (len(extent) - axis_at - 1))

    loudness = one(*split[0])
    for cut in split[1:]:
        loudness = loudness * one(*cut)
    return loudness


def split_up(count, total, most, slope):
    loads = [(1 << 20) // math.isqrt(standing ** slope) + 1 for standing in range(2, count + 1)]
    spare, counts = total - most - (count - 1), [1] * (count - 1)
    while spare > 0:
        candidates = [i for i in range(count - 1) if counts[i] < most]
        pool, budget = sum([loads[i] for i in candidates]), spare
        for i in candidates:
            extra = min(most - counts[i], max(1, budget * loads[i] // pool), spare)
            counts[i] = counts[i] + extra
            spare = spare - extra
    return np.array([most] + counts)


def uneven_parts(rng, amount, total, reach, slope):
    if amount == 2:
        one = jax.random.randint(rng, (), max(1, total - reach), min(reach, total - 1) + 1)
        return jnp.stack([one, total - one])
    tallies = jnp.asarray(split_up(amount, total, reach, slope), jnp.int32)
    twos = (amount - 1) // 2
    giver, taker = tallies[1:1 + 2 * twos:2], tallies[2:2 + 2 * twos:2]
    slack = jnp.minimum(giver - 1, reach - taker)
    moved = jax.random.randint(jax.random.fold_in(rng, 1), (twos,), 0, 1 << 20) % (slack + 1)
    tallies = tallies.at[1:1 + 2 * twos:2].set(giver - moved).at[2:2 + 2 * twos:2].set(taker + moved)
    return tallies[jax.random.permutation(jax.random.fold_in(rng, 2), amount)]


def assign_block(key, own, number, rows, amount, top, most, lean):
    order = jax.random.permutation(key, amount)
    heavy_load, usual = portions_of(amount, rows * top, most, lean, True), portions_of(amount, rows * top, most, lean, False)
    places = jnp.arange(amount)

    def named(sizes, rotation):
        used = int((sizes > 0).sum())
        fixed = max(1, used // 4)
        moved = fixed + (places - fixed + rotation * (used - fixed)) % max(1, amount - fixed)
        return jnp.zeros((amount,), jnp.int32).at[order[jnp.where(places < fixed, places, moved)]].set(jnp.asarray(sizes, jnp.int32))

    sizes = jnp.where(number % 4 == 0, named(heavy_load, number // 4), named(usual, number - number // 4 - 1))
    mixed = jax.random.permutation(jax.random.fold_in(own, 3), amount)
    donor, taker = mixed[0:amount // 2 * 2:2], mixed[1:amount // 2 * 2:2]
    room = jnp.minimum(sizes[donor] - 1, most - sizes[taker]) // 2
    room = jnp.where((donor == order[0]) | (taker == order[0]) | (sizes[taker] == 0), 0, jnp.maximum(room, 0))
    moved = jax.random.randint(jax.random.fold_in(own, 4), (amount // 2,), 0, 1 << 20) % (room + 1)
    sizes = sizes.at[donor].add(-moved).at[taker].add(moved)
    labels = jnp.searchsorted(jnp.cumsum(sizes), jnp.arange(rows * top), side="right").astype(jnp.int32)
    grid = labels.reshape(top, rows).T
    grid = grid[jax.random.permutation(jax.random.fold_in(own, 1), rows)]
    rotation = jax.random.randint(jax.random.fold_in(own, 2), (rows, 1), 0, top)
    return jnp.take_along_axis(grid, (jnp.arange(top)[None, :] + rotation) % top, axis=1)


def portions_of(number_of, total, limit, slope, full):
    weights = [(1 << 20) // math.isqrt(standing ** slope) + 1 for standing in range(1, number_of + 1)]
    largest = limit if full else min(limit, max(-(-total // number_of), total * weights[0] // sum(weights)))
    least = 1 if total - largest >= number_of - 1 else 0
    holding, spare = [largest] + [least] * (number_of - 1), total - largest - least * (number_of - 1)
    while spare > 0:
        candidates = [i for i in range(1, number_of) if holding[i] < largest] or [i for i in range(1, number_of) if holding[i] < limit]
        pool, budget = sum([weights[i] for i in candidates]), spare
        for i in candidates:
            addition = min(limit - holding[i], max(1, budget * weights[i] // pool), spare)
            holding[i] = holding[i] + addition
            spare = spare - addition
    return np.array(holding)


def normal_values(rng, shape, width, limit, pieces=(), held_as=jnp.bfloat16):
    entries = width * jax.random.normal(rng, shape, jnp.float32)
    if pieces:
        entries = entries * levels(rng, shape, pieces, -0.22, 0.18)
    return jnp.clip(entries, -limit, limit).astype(held_as)


def setup_inputs(seed: int = 0) -> dict:
    splits = jax.random.split(jax.random.key(seed), 21)
    tokens = normal_values(splits[0], (SEQUENCES, D), 1.0, 6.0, ((0, 64),))
    attn_gain = jnp.clip(1.0 + 0.18 * jax.random.normal(splits[1], (D,), jnp.float32), 0.1, 1.9)
    query_weight = normal_values(splits[2], (D, HEADS * HEAD_DIM), D ** -0.5, 0.125, ((0, 64), (1, 4)))
    key_weight = normal_values(splits[3], (D, KV_HEADS * HEAD_DIM), D ** -0.5, 0.125, ((0, 64), (1, 4)))
    value_weight = normal_values(splits[4], (D, KV_HEADS * HEAD_DIM), D ** -0.5, 0.125, ((0, 64), (1, 4)))
    break_bias = jnp.clip(-14.0 + 6.0 * jax.random.uniform(splits[5], (HEADS,), jnp.float32) ** levels(splits[5], (HEADS,), ((0, 4),), -0.2, 0.2), -14.0, -8.0)
    cache_keys = normal_values(splits[6], (SEQUENCES, KV_HEADS, CACHE_LEN, HEAD_DIM), 3.0, 18.0, ((0, 64), (1, 4)))
    cache_values = normal_values(splits[7], (SEQUENCES, KV_HEADS, CACHE_LEN, HEAD_DIM), 1.0, 6.0, ((0, 64), (1, 4)))
    lengths = uneven_parts(splits[8], SEQUENCES, SEQUENCES * CACHE_LEN // 2, CACHE_LEN, 2).astype(jnp.int32)
    out_weight = normal_values(splits[9], (HEADS * HEAD_DIM, D), (HEADS * HEAD_DIM // 4) ** -0.5, 0.25, ((0, 4), (1, 64)))
    ffn_gain = jnp.clip(1.0 + 0.18 * jax.random.normal(splits[10], (D,), jnp.float32), 0.1, 1.9)
    branch_gate = normal_values(splits[11], (D,), D ** -0.5, 0.125)
    dense_gate = normal_values(splits[12], (D, DENSE), D ** -0.5, 0.125, ((0, 4), (1, 64)))
    dense_up = normal_values(splits[13], (D, DENSE), D ** -0.5, 0.125, ((0, 4), (1, 64)))
    dense_down = normal_values(splits[14], (DENSE, D), DENSE ** -0.5, 0.0625, ((0, 64), (1, 4)))
    route_ids_keys = jax.random.split(jax.random.fold_in(splits[15], 1), SEQUENCES // SEQS)
    route_ids_turns = jax.random.permutation(jax.random.fold_in(splits[15], 3), SEQUENCES // SEQS)
    route_ids = jax.vmap(lambda own, number: assign_block(jax.random.fold_in(splits[15], 2), own, number, SEQS, EXPERTS, TOP_K, CAP, 2))(route_ids_keys, route_ids_turns).reshape((SEQUENCES, TOP_K))
    route_weights = jnp.clip(jnp.exp(math.log(1.0) - 2.3025851 * jax.random.uniform(splits[16], (SEQUENCES, TOP_K), jnp.float32) ** levels(splits[16], (SEQUENCES, TOP_K), ((0, 64),), -0.2, 0.2)), 0.1, 1.0)
    expert_gate = normal_values(splits[17], (EXPERTS, D, EXPERT_W), (D // 12) ** -0.5, 0.4375, ((0, 64), (2, 4)))
    expert_up = normal_values(splits[18], (EXPERTS, D, EXPERT_W), (D // 12) ** -0.5, 0.4375, ((0, 64), (2, 4)))
    expert_down = normal_values(splits[19], (EXPERTS, EXPERT_W, D), (EXPERT_W * 80) ** -0.5, 0.01953125, ((0, 64), (1, 4)))
    return {"tokens": tokens, "attn_gain": attn_gain, "query_weight": query_weight, "key_weight": key_weight, "value_weight": value_weight, "break_bias": break_bias, "cache_keys": cache_keys, "cache_values": cache_values, "lengths": lengths, "out_weight": out_weight, "ffn_gain": ffn_gain, "branch_gate": branch_gate, "dense_gate": dense_gate, "dense_up": dense_up, "dense_down": dense_down, "route_ids": route_ids, "route_weights": route_weights, "expert_gate": expert_gate, "expert_up": expert_up, "expert_down": expert_down}


norm_eps = 1e-05
clamp_limit = 7.0
swish_alpha = 1.702

def rms_scale(values, gain):
    return values * lax.rsqrt(lax.optimization_barrier(jnp.mean(values * values, axis=-1, keepdims=True)) + norm_eps) * gain

def clamped_unit(gate_pre, up_pre):
    gate_c = jnp.minimum(gate_pre, clamp_limit)
    up_c = jnp.clip(up_pre, -clamp_limit, clamp_limit)
    return (up_c + 1.0) * gate_c * jax.nn.sigmoid(swish_alpha * gate_c)

def reference(tokens, attn_gain, query_weight, key_weight, value_weight, break_bias, cache_keys, cache_values, lengths, out_weight, ffn_gain, branch_gate, dense_gate, dense_up, dense_down, route_ids, route_weights, expert_gate, expert_up, expert_down):
    normed = rms_scale(tokens.astype(jnp.float32), attn_gain).astype(jnp.bfloat16)
    queries = jnp.dot(normed, query_weight, preferred_element_type=jnp.float32).astype(jnp.bfloat16)
    new_keys = jnp.dot(normed, key_weight, preferred_element_type=jnp.float32).astype(jnp.bfloat16)
    new_values = jnp.dot(normed, value_weight, preferred_element_type=jnp.float32).astype(jnp.bfloat16)
    group_size = HEADS // KV_HEADS
    query_heads = queries.reshape(SEQUENCES, KV_HEADS, group_size, HEAD_DIM)
    head_bias = break_bias.reshape(KV_HEADS, group_size)
    positions = jnp.arange(CACHE_LEN, dtype=jnp.int32)

    def one_sequence(packed):
        query_rows, key_rows, value_rows, length_now = packed
        scores = jnp.einsum('grd,gld->grl', query_rows.astype(jnp.float32), key_rows.astype(jnp.float32))
        scores = scores * HEAD_DIM ** (-0.5) + head_bias[:, :, None]
        inside = (positions < length_now)[None, None, :]
        log_keep = jnp.where(inside, jax.nn.log_sigmoid(-scores), 0.0)
        between = lax.cumsum(log_keep, axis=2, reverse=True) - log_keep
        weights = jnp.where(inside, jnp.exp(jax.nn.log_sigmoid(scores) + between), 0.0).astype(jnp.bfloat16)
        return jnp.einsum('grl,gld->grd', weights.astype(jnp.float32), value_rows.astype(jnp.float32)).astype(jnp.bfloat16)
    attended = lax.map(one_sequence, (query_heads, cache_keys, cache_values, lengths))
    attended = attended.reshape(SEQUENCES, HEADS * HEAD_DIM)
    mixed = jnp.dot(attended, out_weight, preferred_element_type=jnp.float32).astype(jnp.bfloat16)
    resid = tokens.astype(jnp.float32) + mixed.astype(jnp.float32)
    normed2 = rms_scale(resid, ffn_gain).astype(jnp.bfloat16)
    slot_count = N_EP * CAP
    token_ids = jnp.arange(SEQUENCES, dtype=jnp.int32)

    def per_expert(expert_sum, expert):
        route_hits = route_ids == expert
        chosen = jnp.any(route_hits, axis=1)
        scale_sum = lax.optimization_barrier(jnp.sum(jnp.where(route_hits, route_weights, 0.0), axis=1))
        place_index = jnp.cumsum(chosen.astype(jnp.int32)) - 1
        target = jnp.where(chosen, place_index, slot_count).astype(jnp.int32)
        row_index = jnp.zeros((slot_count + 1,), jnp.int32).at[target].set(token_ids)[:slot_count]
        picked_rows = normed2[row_index]
        gate_pre = jnp.dot(picked_rows, expert_gate[expert], preferred_element_type=jnp.float32)
        up_pre = jnp.dot(picked_rows, expert_up[expert], preferred_element_type=jnp.float32)
        activation = clamped_unit(gate_pre, up_pre).astype(jnp.bfloat16)
        expert_rows = jnp.dot(activation, expert_down[expert], preferred_element_type=jnp.float32).astype(jnp.bfloat16)
        slot_live = jnp.arange(slot_count, dtype=jnp.int32) < jnp.sum(chosen.astype(jnp.int32))
        row_scale = jnp.where(slot_live, scale_sum[row_index], 0.0)
        return (expert_sum.at[row_index].add(row_scale[:, None] * expert_rows.astype(jnp.float32)), None)
    expert_sum, unused_out = lax.scan(per_expert, jnp.zeros((SEQUENCES, D), jnp.float32), jnp.arange(EXPERTS, dtype=jnp.int32))
    gate_part = jnp.dot(normed2, dense_gate, preferred_element_type=jnp.float32)
    up_part = jnp.dot(normed2, dense_up, preferred_element_type=jnp.float32)
    hidden_units = (jax.nn.silu(gate_part) * up_part).astype(jnp.bfloat16)
    dense_out = jnp.dot(hidden_units, dense_down, preferred_element_type=jnp.float32)
    branch_scale = jax.nn.sigmoid(jnp.dot(normed2, branch_gate, preferred_element_type=jnp.float32))
    layer_out = (resid + expert_sum + branch_scale[:, None] * dense_out).astype(jnp.bfloat16)
    return (layer_out, new_keys, new_values)
```

```python
import functools

import jax
import jax.numpy as jnp
from jax import lax
from jax.experimental import pallas as pl
from jax.experimental.pallas import tpu as pltpu
from jax.sharding import Mesh
from jax.sharding import PartitionSpec as P

EP = ("z", "x", "c")
NZ, NX, NC, NT = 8, 4, 2, 4
NJ = NX * NC

norm_eps = 1e-05
clamp_limit = 7.0
swish_alpha = 1.702

BF = jnp.bfloat16
F32 = jnp.float32
MESH_IDS = pl.DeviceIdType.MESH


def dot(a, b):
    return jnp.dot(a, b, preferred_element_type=F32)


def dot_nt(a, b):
    return lax.dot_general(a, b, (((1,), (1,)), ((), ())), preferred_element_type=F32)


def iota(shape, dim):
    return lax.broadcasted_iota(jnp.int32, shape, dim)


def one_if(mask):
    return jnp.where(mask, 1.0, 0.0)


def kernel(
    tokens,
    attn_gain,
    wq_in,
    wk_in,
    wv_in,
    bias,
    keys_hbm,
    values_hbm,
    lengths,
    wo_in,
    ffn_gain,
    branch_gate,
    dgate_hbm,
    dup_hbm,
    ddown_hbm,
    route_ids,
    route_weights,
    egate_hbm,
    eup_hbm,
    edown_hbm,
    layer_out,
    new_keys,
    new_values,
    keys,
    values,
    egate,
    eup,
    edown,
    dgate,
    dup,
    ddown,
    wq,
    wk,
    wv,
    wo,
    nsend,
    nslab,
    qsend,
    qrecv,
    scores,
    q64,
    att64,
    att_all,
    wd_all,
    po,
    mx_send,
    mx_recv,
    resid,
    xs,
    row_send,
    row_recv,
    pd_send,
    pd_recv,
    hid,
    pe_send,
    pe_recv,
    er,
    er_recv,
    dense_part,
    fin_send,
    fin_recv,
    local_sem,
    kv_sem,
    z_send,
    z_recv,
    j_send,
    j_recv,
    t_send,
    t_recv,
):
    mz = lax.axis_index("z")
    mxx = lax.axis_index("x")
    mc = lax.axis_index("c")
    mt = lax.axis_index("tp")
    mj = mxx * NC + mc

    def zpeer(d):
        return lax.rem(mz + d, NZ)

    def jpeer(d):
        return lax.rem(mj + d, NJ)

    def tpeer(d):
        return lax.rem(mt + d, NT)

    def zdev(d):
        return {"z": zpeer(d)}

    def jdev(d):
        j = jpeer(d)
        return {"x": lax.div(j, NC), "c": lax.rem(j, NC)}

    def tdev(d):
        return {"tp": tpeer(d)}

    def remote(src, dst, ssem, rsem, dev):
        return pltpu.make_async_remote_copy(
            src_ref=src,
            dst_ref=dst,
            send_sem=ssem,
            recv_sem=rsem,
            device_id=dev,
            device_id_type=MESH_IDS,
        )

    started = []

    def exchange(n, make):
        copies = [make(d) for d in range(1, n)]
        for copy in copies:
            copy.start()
        started.extend(copies)
        return copies

    def arrived(copies):
        for copy in copies:
            copy.wait_recv()

    locals_ = []
    kv_copies = []
    for s in range(0, 16, 2):
        kv_copies.append(
            pltpu.make_async_copy(
                keys_hbm.at[pl.ds(s, 2), 0], keys.at[pl.ds(s, 2)], kv_sem.at[s]
            )
        )
        kv_copies.append(
            pltpu.make_async_copy(
                values_hbm.at[pl.ds(s, 2), 0], values.at[pl.ds(s, 2)], kv_sem.at[s + 1]
            )
        )
    for copy in kv_copies:
        copy.start()
    dense_col = pl.ds(pl.multiple_of(mj * 128, 128), 128)
    locals_.append(pltpu.make_async_copy(dgate_hbm, dgate.at[:, dense_col], local_sem.at[0]))
    locals_.append(pltpu.make_async_copy(dup_hbm, dup.at[:, dense_col], local_sem.at[1]))
    locals_.append(pltpu.make_async_copy(ddown_hbm, ddown.at[dense_col], local_sem.at[2]))
    locals_.append(pltpu.make_async_copy(egate_hbm.at[0], egate, local_sem.at[3]))
    locals_.append(pltpu.make_async_copy(eup_hbm.at[0], eup, local_sem.at[4]))
    locals_.append(pltpu.make_async_copy(edown_hbm.at[0], edown, local_sem.at[5]))
    for copy in locals_:
        copy.start()

    barrier = pltpu.get_barrier_semaphore()
    for d in range(1, NJ):
        pl.semaphore_signal(barrier, inc=1, device_id=jdev(d), device_id_type=MESH_IDS)
    for d in range(1, NZ):
        pl.semaphore_signal(barrier, inc=1, device_id=zdev(d), device_id_type=MESH_IDS)
    for d in range(1, NT):
        pl.semaphore_signal(barrier, inc=1, device_id=tdev(d), device_id_type=MESH_IDS)

    tok = tokens[...].astype(F32)
    normed = (
        tok * lax.rsqrt(jnp.mean(tok * tok, axis=-1, keepdims=True) + norm_eps) * attn_gain[...]
    ).astype(BF)
    for z in range(NZ):
        nsend[z] = normed[:, 256 * z : 256 * (z + 1)]

    ids = route_ids[...]
    rws = route_weights[...]
    lane_expert = lax.shift_right_logical(iota((16, 128), 1), 1)
    named = jnp.zeros((16, 128), F32)
    weighed = jnp.zeros((16, 128), F32)
    for k in range(4):
        hit = ids[:, k : k + 1] == lane_expert
        named = named + one_if(hit)
        weighed = weighed + jnp.where(hit, rws[:, k : k + 1], 0.0)
    earlier = one_if(iota((16, 16), 1) < iota((16, 16), 0)).astype(BF)
    rank = dot(earlier, named.astype(BF))
    lane_rank = jnp.bitwise_and(iota((16, 128), 1), 1).astype(F32)
    wd_all[mz] = jnp.where(rank == lane_rank, weighed, 0.0)

    pl.semaphore_wait(barrier, NJ + NZ + NT - 3)

    c_wq = exchange(
        NJ, lambda d: remote(wq_in, wq.at[mj], j_send.at[0, d], j_recv.at[0, d], jdev(d))
    )
    c_wk = exchange(
        NJ, lambda d: remote(wk_in, wk.at[mj], j_send.at[1, d], j_recv.at[1, d], jdev(d))
    )
    c_wv = exchange(
        NJ, lambda d: remote(wv_in, wv.at[mj], j_send.at[2, d], j_recv.at[2, d], jdev(d))
    )
    c_n = exchange(
        NZ,
        lambda d: remote(
            nsend.at[zpeer(d)], nslab.at[mz], z_send.at[0, d], z_recv.at[0, d], zdev(d)
        ),
    )
    c_wd = exchange(
        NZ,
        lambda d: remote(
            wd_all.at[mz], wd_all.at[mz], z_send.at[1, d], z_recv.at[1, d], zdev(d)
        ),
    )
    c_wo = exchange(
        NJ, lambda d: remote(wo_in, wo.at[mj], j_send.at[3, d], j_recv.at[3, d], jdev(d))
    )
    c_dg = exchange(
        NJ,
        lambda d: remote(
            dgate_hbm, dgate.at[:, dense_col], j_send.at[4, d], j_recv.at[4, d], jdev(d)
        ),
    )
    c_du = exchange(
        NJ,
        lambda d: remote(
            dup_hbm, dup.at[:, dense_col], j_send.at[5, d], j_recv.at[5, d], jdev(d)
        ),
    )
    c_dd = exchange(
        NJ,
        lambda d: remote(
            ddown_hbm, ddown.at[dense_col], j_send.at[6, d], j_recv.at[6, d], jdev(d)
        ),
    )
    wq[mj] = wq_in[...]
    wk[mj] = wk_in[...]
    wv[mj] = wv_in[...]
    wo[mj] = wo_in[...]
    nslab[mz] = nsend[mz]

    arrived(c_n)
    arrived(c_wq)
    arrived(c_wk)
    arrived(c_wv)
    slab = nslab[...].reshape(128, 256)
    qsend[:, :, 0:512] = dot(slab, wq[...].reshape(256, 512)).astype(BF).reshape(NZ, 16, 512)
    qsend[:, :, 512:640] = dot(slab, wk[...].reshape(256, 128)).astype(BF).reshape(NZ, 16, 128)
    qsend[:, :, 640:768] = dot(slab, wv[...].reshape(256, 128)).astype(BF).reshape(NZ, 16, 128)
    c_q = exchange(
        NZ,
        lambda d: remote(
            qsend.at[zpeer(d)], qrecv.at[mz], z_send.at[2, d], z_recv.at[2, d], zdev(d)
        ),
    )
    qrecv[mz] = qsend[mz]
    arrived(c_q)
    total = qrecv[0].astype(F32)
    for z in range(1, NZ):
        total = total + qrecv[z].astype(F32)
    total = total.astype(BF)
    new_keys[...] = total[:, 512:640]
    new_values[...] = total[:, 640:768]

    q_rows = jnp.zeros((64, 128), F32)
    for h in range(4):
        spread = one_if(iota((64, 16), 0) == 4 * iota((64, 16), 1) + h).astype(BF)
        q_rows = q_rows + dot(spread, total[:, 128 * h : 128 * (h + 1)])
    q64[...] = q_rows
    for copy in kv_copies:
        copy.wait()
    first = iota((8, 128), 0) < 4
    for p in range(8):
        q8 = q64[8 * p : 8 * p + 8]
        qa = jnp.where(first, q8, 0.0).astype(BF)
        qb = jnp.where(first, 0.0, q8).astype(BF)
        scores[8 * p : 8 * p + 8] = dot_nt(qa, keys[2 * p]) + dot_nt(qb, keys[2 * p + 1])

    row = iota((64, 1), 0)
    head = jnp.bitwise_and(row, 3)
    seq = lax.shift_right_logical(row, 2)
    bias_col = jnp.zeros((64, 1), F32)
    for h in range(4):
        bias_col = jnp.where(head == h, bias[h], bias_col)
    len_col = jnp.zeros((64, 1), jnp.int32)
    for s in range(16):
        len_col = jnp.where(seq == s, lengths[s], len_col)
    after = one_if(iota((128, 128), 0) > iota((128, 128), 1)).astype(BF)
    carry = jnp.zeros((64, 1), F32)
    for b in reversed(range(8)):
        cols = slice(128 * b, 128 * (b + 1))
        zz = scores[:, cols] * (128 ** (-0.5)) + bias_col
        inside = (iota((64, 128), 1) + 128 * b) < len_col
        soft = jnp.log1p(jnp.exp(-jnp.abs(zz)))
        keep = jnp.where(inside, jnp.minimum(-zz, 0.0) - soft, 0.0)
        take = jnp.minimum(zz, 0.0) - soft
        k1 = keep.astype(BF)
        r1 = keep - k1.astype(F32)
        k2 = r1.astype(BF)
        k3 = (r1 - k2.astype(F32)).astype(BF)
        between = dot(k1, after) + dot(k2, after) + dot(k3, after) + carry
        carry = between[:, 0:1] + keep[:, 0:1]
        scores[:, cols] = jnp.where(inside, jnp.exp(take + between), 0.0)

    for p in range(8):
        w8 = scores[8 * p : 8 * p + 8].astype(BF)
        att64[8 * p : 8 * p + 8] = jnp.where(
            first, dot(w8, values[2 * p]), dot(w8, values[2 * p + 1])
        )
    att_rows = att64[...].astype(BF)
    for h in range(4):
        pick = one_if(iota((16, 64), 1) == 4 * iota((16, 64), 0) + h).astype(BF)
        att_all[mz, :, 128 * h : 128 * (h + 1)] = dot(pick, att_rows).astype(BF)

    c_a = exchange(
        NZ,
        lambda d: remote(
            att_all.at[mz], att_all.at[mz], z_send.at[3, d], z_recv.at[3, d], zdev(d)
        ),
    )
    arrived(c_wo)
    arrived(c_a)
    po[mt] = dot_nt(att_all[...].reshape(128, 512), wo[...].reshape(256, 512)).astype(BF)
    c_po = exchange(
        NT, lambda d: remote(po.at[mt], po.at[mt], t_send.at[0, d], t_recv.at[0, d], tdev(d))
    )
    arrived(c_po)
    mixed = po[0].astype(F32)
    for t in range(1, NT):
        mixed = mixed + po[t].astype(F32)
    mx_send[...] = mixed.astype(BF).reshape(NZ, 16, 256)
    c_mx = exchange(
        NZ,
        lambda d: remote(
            mx_send.at[zpeer(d)], mx_recv.at[mz], z_send.at[4, d], z_recv.at[4, d], zdev(d)
        ),
    )
    mx_recv[mz] = mx_send[mz]
    arrived(c_mx)
    for z in range(NZ):
        cols = slice(256 * z, 256 * (z + 1))
        resid[:, cols] = tokens[:, cols].astype(F32) + mx_recv[z].astype(F32)
    res = resid[...]
    xs[mz] = (
        res * lax.rsqrt(jnp.mean(res * res, axis=-1, keepdims=True) + norm_eps) * ffn_gain[...]
    ).astype(BF)

    c_x = exchange(
        NZ, lambda d: remote(xs.at[mz], xs.at[mz], z_send.at[5, d], z_recv.at[5, d], zdev(d))
    )
    arrived(c_wd)
    slot_of_row = 16 * mz + 2 * lax.shift_right_logical(iota((128, 128), 0), 4)
    slot_of_row = slot_of_row + jnp.bitwise_and(iota((128, 128), 0), 1)
    spread = one_if(slot_of_row == iota((128, 128), 1)).astype(BF)
    row_z = jnp.bitwise_and(lax.shift_right_logical(iota((128, 128), 0), 1), 7)
    own_z = row_z == lax.shift_right_logical(iota((128, 128), 1), 4)
    wd = wd_all[...].reshape(128, 128)
    wd_hi = wd.astype(BF)
    wd_lo = (wd - wd_hi.astype(F32)).astype(BF)
    filled = one_if(wd > 0.0).astype(BF)
    dispatch = jnp.where(own_z, dot_nt(spread, filled), 0.0).astype(BF)
    row_z_t = jnp.bitwise_and(lax.shift_right_logical(iota((128, 128), 1), 1), 7)
    own_z_t = row_z_t == lax.shift_right_logical(iota((128, 128), 0), 4)
    comb_hi = jnp.where(own_z_t, dot_nt(wd_hi, spread), 0.0).astype(BF)
    comb_lo = jnp.where(own_z_t, dot_nt(wd_lo, spread), 0.0).astype(BF)

    arrived(c_x)
    for b in range(4):
        cols = slice(512 * b, 512 * (b + 1))
        row_send[:, :, cols] = (
            dot(dispatch, xs[:, :, cols].reshape(128, 512)).astype(BF).reshape(NJ, 16, 512)
        )
    c_row = exchange(
        NJ,
        lambda d: remote(
            row_send.at[jpeer(d)], row_recv.at[mj], j_send.at[7, d], j_recv.at[7, d], jdev(d)
        ),
    )
    row_recv[mj] = row_send[mj]

    for copy in locals_:
        copy.wait()
    arrived(c_dg)
    arrived(c_du)
    own_cols = pl.ds(pl.multiple_of(mt * 512, 512), 512)
    x_own = xs[:, :, own_cols].reshape(128, 512)
    for t in range(NT):
        cols = slice(256 * t, 256 * (t + 1))
        pd_send[t, :, 0:256] = dot(x_own, dgate[:, cols]).astype(BF)
        pd_send[t, :, 256:512] = dot(x_own, dup[:, cols]).astype(BF)
    c_pd = exchange(
        NT,
        lambda d: remote(
            pd_send.at[tpeer(d)], pd_recv.at[mt], t_send.at[1, d], t_recv.at[1, d], tdev(d)
        ),
    )
    pd_recv[mt] = pd_send[mt]
    x_all = xs[...].reshape(128, 2048).astype(F32)
    branch = jax.nn.sigmoid(jnp.sum(x_all * branch_gate[...], axis=-1, keepdims=True))
    arrived(c_pd)
    pre = pd_recv[0].astype(F32)
    for t in range(1, NT):
        pre = pre + pd_recv[t].astype(F32)
    gate_d = pre[:, 0:256]
    hid[mt] = (gate_d * jax.nn.sigmoid(gate_d) * pre[:, 256:512]).astype(BF)
    c_h = exchange(
        NT, lambda d: remote(hid.at[mt], hid.at[mt], t_send.at[2, d], t_recv.at[2, d], tdev(d))
    )

    arrived(c_row)
    rows = row_recv[...].reshape(128, 2048)
    gate_c = jnp.minimum(dot(rows, egate[...]), clamp_limit)
    up_c = jnp.clip(dot(rows, eup[...]), -clamp_limit, clamp_limit)
    unit = ((up_c + 1.0) * gate_c * jax.nn.sigmoid(swish_alpha * gate_c)).astype(BF)
    for t in range(NT):
        pe_send[t] = dot(unit, edown[:, 512 * t : 512 * (t + 1)]).astype(BF)
    c_pe = exchange(
        NT,
        lambda d: remote(
            pe_send.at[tpeer(d)], pe_recv.at[mt], t_send.at[3, d], t_recv.at[3, d], tdev(d)
        ),
    )
    pe_recv[mt] = pe_send[mt]

    arrived(c_h)
    arrived(c_dd)
    down = dot(hid[0], ddown[0:256])
    for t in range(1, NT):
        down = down + dot(hid[t], ddown[256 * t : 256 * (t + 1)])
    dense_part[...] = down * branch

    arrived(c_pe)
    total_e = pe_recv[0].astype(F32)
    for t in range(1, NT):
        total_e = total_e + pe_recv[t].astype(F32)
    er[...] = total_e.astype(BF).reshape(NJ, 16, 512)
    c_er = exchange(
        NJ,
        lambda d: remote(
            er.at[jpeer(d)], er_recv.at[mj], j_send.at[8, d], j_recv.at[8, d], jdev(d)
        ),
    )
    er_recv[mj] = er[mj]
    arrived(c_er)
    back = er_recv[...].reshape(128, 512)
    fin_send[...] = (
        (dot(comb_hi, back) + dot(comb_lo, back) + dense_part[...]).astype(BF).reshape(NZ, 16, 512)
    )
    c_f = exchange(
        NZ,
        lambda d: remote(
            fin_send.at[zpeer(d)], fin_recv.at[mz], z_send.at[6, d], z_recv.at[6, d], zdev(d)
        ),
    )
    fin_recv[mz] = fin_send[mz]
    arrived(c_f)
    final = resid[:, own_cols]
    for z in range(NZ):
        final = final + fin_recv[z].astype(F32)
    layer_out[...] = final.astype(BF)

    for copy in started:
        copy.wait_send()


def body(
    tokens,
    attn_gain,
    query_weight,
    key_weight,
    value_weight,
    break_bias,
    cache_keys,
    cache_values,
    lengths,
    out_weight,
    ffn_gain,
    branch_gate,
    dense_gate,
    dense_up,
    dense_down,
    route_ids,
    route_weights,
    expert_gate,
    expert_up,
    expert_down,
):
    vm = pl.BlockSpec(memory_space=pltpu.VMEM)
    sm = pl.BlockSpec(memory_space=pltpu.SMEM)
    hbm = pl.BlockSpec(memory_space=pl.ANY)
    V = pltpu.VMEM
    return tuple(
        pl.pallas_call(
            kernel,
            name="layer",
            out_shape=(
                jax.ShapeDtypeStruct((16, 512), BF),
                jax.ShapeDtypeStruct((16, 128), BF),
                jax.ShapeDtypeStruct((16, 128), BF),
            ),
            in_specs=[
                vm,
                vm,
                vm,
                vm,
                vm,
                sm,
                hbm,
                hbm,
                sm,
                vm,
                vm,
                vm,
                hbm,
                hbm,
                hbm,
                vm,
                vm,
                hbm,
                hbm,
                hbm,
            ],
            out_specs=(vm, vm, vm),
            scratch_shapes=[
                V((16, 1024, 128), BF),
                V((16, 1024, 128), BF),
                V((2048, 256), BF),
                V((2048, 256), BF),
                V((256, 2048), BF),
                V((512, 1024), BF),
                V((512, 1024), BF),
                V((1024, 512), BF),
                V((NJ, 32, 512), BF),
                V((NJ, 32, 128), BF),
                V((NJ, 32, 128), BF),
                V((NJ, 32, 512), BF),
                V((NZ, 16, 256), BF),
                V((NZ, 16, 256), BF),
                V((NZ, 16, 768), BF),
                V((NZ, 16, 768), BF),
                V((64, 1024), F32),
                V((64, 128), F32),
                V((64, 128), F32),
                V((NZ, 16, 512), BF),
                V((NZ, 16, 128), F32),
                V((NT, 128, 256), BF),
                V((NZ, 16, 256), BF),
                V((NZ, 16, 256), BF),
                V((16, 2048), F32),
                V((NZ, 16, 2048), BF),
                V((NJ, 16, 2048), BF),
                V((NJ, 16, 2048), BF),
                V((NT, 128, 512), BF),
                V((NT, 128, 512), BF),
                V((NT, 128, 256), BF),
                V((NT, 128, 512), BF),
                V((NT, 128, 512), BF),
                V((NJ, 16, 512), BF),
                V((NJ, 16, 512), BF),
                V((128, 512), F32),
                V((NZ, 16, 512), BF),
                V((NZ, 16, 512), BF),
                pltpu.SemaphoreType.DMA((6,)),
                pltpu.SemaphoreType.DMA((16,)),
                pltpu.SemaphoreType.DMA((7, NZ)),
                pltpu.SemaphoreType.DMA((7, NZ)),
                pltpu.SemaphoreType.DMA((9, NJ)),
                pltpu.SemaphoreType.DMA((9, NJ)),
                pltpu.SemaphoreType.DMA((4, NT)),
                pltpu.SemaphoreType.DMA((4, NT)),
            ],
            compiler_params=pltpu.CompilerParams(
                collective_id=0,
                has_side_effects=True,
                vmem_limit_bytes=60 * 1024 * 1024,
            ),
        )(
            tokens,
            attn_gain.reshape(1, -1),
            query_weight,
            key_weight,
            value_weight,
            break_bias,
            cache_keys,
            cache_values,
            lengths,
            out_weight.T,
            ffn_gain.reshape(1, -1),
            branch_gate.astype(F32).reshape(1, -1),
            dense_gate,
            dense_up,
            dense_down,
            route_ids,
            route_weights,
            expert_gate,
            expert_up,
            expert_down,
        )
    )


def solution(mesh):
    split = Mesh(mesh.devices.reshape(NZ, NX, NC, NT), ("z", "x", "c", "tp"))
    return jax.shard_map(
        body,
        mesh=split,
        in_specs=(
            P(EP, None),
            P(),
            P(EP, "tp"),
            P(EP, "tp"),
            P(EP, "tp"),
            P("tp"),
            P(EP, "tp", None, None),
            P(EP, "tp", None, None),
            P(EP),
            P("tp", EP),
            P(),
            P(),
            P("tp", EP),
            P("tp", EP),
            P(EP, "tp"),
            P(EP, None),
            P(EP, None),
            P(EP, None, "tp"),
            P(EP, None, "tp"),
            P(EP, "tp", None),
        ),
        out_specs=(P(EP, "tp"), P(EP, "tp"), P(EP, "tp")),
        check_vma=False,
    )
```

```python
import functools

import jax
import jax.numpy as jnp
from jax import lax
from jax.experimental import pallas as pl
from jax.experimental.pallas import tpu as pltpu
from jax.sharding import Mesh
from jax.sharding import PartitionSpec as P

EP = ("z", "x", "c")
NZ, NX, NC, NT = 8, 4, 2, 4
NJ = NX * NC

norm_eps = 1e-05
clamp_limit = 7.0
swish_alpha = 1.702

BF = jnp.bfloat16
F32 = jnp.float32
MESH_IDS = pl.DeviceIdType.MESH


def dot(a, b):
    return jnp.dot(a, b, preferred_element_type=F32)


def dot_nt(a, b):
    return lax.dot_general(a, b, (((1,), (1,)), ((), ())), preferred_element_type=F32)


def iota(shape, dim):
    return lax.broadcasted_iota(jnp.int32, shape, dim)


def one_if(mask):
    return jnp.where(mask, 1.0, 0.0)


Z_ORDER = (4, 3, 5, 2, 6, 1, 7)
J_ORDER = (4, 3, 5, 2, 6, 1, 7)
T_ORDER = (2, 1, 3)


def kernel(
    tokens_in,
    attn_gain_in,
    wq_hbm,
    wk_hbm,
    wv_hbm,
    bias,
    keys_hbm,
    values_hbm,
    lengths,
    wo_hbm,
    ffn_gain_in,
    branch_gate_in,
    dgate_hbm,
    dup_hbm,
    ddown_hbm,
    route_ids_in,
    route_weights_in,
    egate_hbm,
    eup_hbm,
    edown_hbm,
    out,
    tokens,
    attn_gain,
    wq_in,
    wk_in,
    wv_in,
    wo_in,
    ffn_gain,
    branch_gate,
    route_ids,
    route_weights,
    keys,
    values,
    egate,
    eup,
    edown,
    dgate,
    dup,
    ddown,
    wq,
    wk,
    wv,
    wo,
    nsend,
    nslab,
    qsend,
    qrecv,
    scores,
    q64,
    att64,
    att_all,
    wd_all,
    tok_all,
    po_send,
    po_recv,
    mixed,
    xs,
    row_send,
    row_recv,
    pd_send,
    pd_recv,
    hid,
    pe_send,
    pe_recv,
    er,
    er_recv,
    dense_part,
    fin_send,
    fin_recv,
    in_sem,
    local_sem,
    kv_sem,
    z_send,
    z_recv,
    j_send,
    j_recv,
    t_send,
    t_recv,
    ft_send,
    ft_recv,
    fm_send,
    fm_recv,
):
    mz = lax.axis_index("z")
    mxx = lax.axis_index("x")
    mc = lax.axis_index("c")
    mt = lax.axis_index("tp")
    mj = mxx * NC + mc

    def zpeer(d):
        return lax.rem(mz + d, NZ)

    def zsource(d):
        return lax.rem(mz + NZ - d, NZ)

    def jpeer(d):
        return lax.rem(mj + d, NJ)

    def tpeer(d):
        return lax.rem(mt + d, NT)

    def zdev(d):
        return {"z": zpeer(d)}

    def jdev(d):
        j = jpeer(d)
        return {"x": lax.div(j, NC), "c": lax.rem(j, NC)}

    def tdev(d):
        return {"tp": tpeer(d)}

    def remote(src, dst, ssem, rsem, dev):
        return pltpu.make_async_remote_copy(
            src_ref=src,
            dst_ref=dst,
            send_sem=ssem,
            recv_sem=rsem,
            device_id=dev,
            device_id_type=MESH_IDS,
        )

    started = []

    def exchange(order, make):
        copies = [make(d) for d in order]
        for copy in copies:
            copy.start()
        started.extend(copies)
        return copies

    def arrived(copies):
        for copy in reversed(copies):
            copy.wait_recv()

    barrier = pltpu.get_barrier_semaphore()
    for d in Z_ORDER:
        pl.semaphore_signal(barrier, inc=1, device_id=zdev(d), device_id_type=MESH_IDS)
    for d in J_ORDER:
        pl.semaphore_signal(barrier, inc=1, device_id=jdev(d), device_id_type=MESH_IDS)
    for d in T_ORDER:
        pl.semaphore_signal(barrier, inc=1, device_id=tdev(d), device_id_type=MESH_IDS)

    inputs = [
        pltpu.make_async_copy(src, dst, in_sem.at[k])
        for k, (src, dst) in enumerate(
            (
                (tokens_in, tokens),
                (attn_gain_in, attn_gain),
                (wq_hbm, wq_in),
                (wk_hbm, wk_in),
                (wv_hbm, wv_in),
                (route_ids_in, route_ids),
                (route_weights_in, route_weights),
                (wo_hbm, wo_in),
                (ffn_gain_in, ffn_gain),
                (branch_gate_in, branch_gate),
            )
        )
    ]
    for copy in inputs:
        copy.start()
    kv_copies = []
    for s in range(0, 16, 2):
        kv_copies.append(
            pltpu.make_async_copy(
                keys_hbm.at[pl.ds(s, 2), 0], keys.at[pl.ds(s, 2)], kv_sem.at[s]
            )
        )
    for s in range(0, 16, 2):
        kv_copies.append(
            pltpu.make_async_copy(
                values_hbm.at[pl.ds(s, 2), 0], values.at[pl.ds(s, 2)], kv_sem.at[s + 1]
            )
        )
    for copy in kv_copies:
        copy.start()
    dense_col = pl.ds(pl.multiple_of(mj * 128, 128), 128)
    locals_ = [
        pltpu.make_async_copy(dgate_hbm, dgate.at[:, dense_col], local_sem.at[0]),
        pltpu.make_async_copy(dup_hbm, dup.at[:, dense_col], local_sem.at[1]),
        pltpu.make_async_copy(ddown_hbm, ddown.at[dense_col], local_sem.at[2]),
        pltpu.make_async_copy(egate_hbm.at[0], egate, local_sem.at[3]),
        pltpu.make_async_copy(eup_hbm.at[0], eup, local_sem.at[4]),
        pltpu.make_async_copy(edown_hbm.at[0], edown, local_sem.at[5]),
    ]
    for copy in locals_:
        copy.start()

    for copy in inputs[0:2]:
        copy.wait()
    tok = tokens[...].astype(F32)
    normed = (
        tok * lax.rsqrt(jnp.mean(tok * tok, axis=-1, keepdims=True) + norm_eps) * attn_gain[...]
    ).astype(BF)
    for z in range(NZ):
        nsend[z] = normed[:, 256 * z : 256 * (z + 1)]
    for copy in inputs[2:]:
        copy.wait()

    pl.semaphore_wait(barrier, NJ + NZ + NT - 3)

    def chunk_of(src, dst, k, lo, hi):
        return exchange(
            J_ORDER,
            lambda d: remote(
                src.at[:, lo:hi],
                dst.at[mj, :, lo:hi],
                j_send.at[k, d],
                j_recv.at[k, d],
                jdev(d),
            ),
        )

    c_wa = chunk_of(wq_in, wq, 0, 0, 256)
    c_n = exchange(
        Z_ORDER,
        lambda d: remote(
            nsend.at[zpeer(d)], nslab.at[mz], z_send.at[0, d], z_recv.at[0, d], zdev(d)
        ),
    )
    c_wb = chunk_of(wq_in, wq, 1, 256, 512)
    c_wk = chunk_of(wk_in, wk, 2, 0, 128)
    c_wv = chunk_of(wv_in, wv, 9, 0, 128)
    c_wo = exchange(
        J_ORDER, lambda d: remote(wo_in, wo.at[mj], j_send.at[3, d], j_recv.at[3, d], jdev(d))
    )
    c_dg = exchange(
        J_ORDER,
        lambda d: remote(
            dgate_hbm, dgate.at[:, dense_col], j_send.at[4, d], j_recv.at[4, d], jdev(d)
        ),
    )
    c_du = exchange(
        J_ORDER,
        lambda d: remote(
            dup_hbm, dup.at[:, dense_col], j_send.at[5, d], j_recv.at[5, d], jdev(d)
        ),
    )
    c_dd = exchange(
        J_ORDER,
        lambda d: remote(
            ddown_hbm, ddown.at[dense_col], j_send.at[6, d], j_recv.at[6, d], jdev(d)
        ),
    )
    wq[mj] = wq_in[...]
    wk[mj] = wk_in[...]
    wv[mj] = wv_in[...]
    wo[mj] = wo_in[...]
    nslab[mz] = nsend[mz]
    tok_all[mz] = tokens[...]

    row_expert = lax.shift_right_logical(iota((128, 16), 0), 1)
    named = jnp.zeros((128, 16), F32)
    weighed = jnp.zeros((128, 16), F32)
    for k in range(4):
        hit = route_ids[k : k + 1, :] == row_expert
        named = named + one_if(hit)
        weighed = weighed + jnp.where(hit, route_weights[k : k + 1, :], 0.0)
    earlier = one_if(iota((16, 16), 0) < iota((16, 16), 1)).astype(BF)
    rank = dot(named.astype(BF), earlier)
    row_rank = jnp.bitwise_and(iota((128, 16), 0), 1).astype(F32)
    slots = jnp.where(rank == row_rank, weighed, 0.0)
    wd_all[mz] = jnp.concatenate([slots, jnp.zeros((128, 112), F32)], axis=1).T[0:16]

    def q_chunk(k, weight, lo, hi, at):
        width = hi - lo
        cols = slice(at, at + width)
        qsend[:, :, cols] = (
            dot(nslab[...].reshape(128, 256), weight[:, :, lo:hi].reshape(256, width))
            .astype(BF)
            .reshape(NZ, 16, width)
        )

    def q_exchange(k, lo, hi):
        copies = exchange(
            Z_ORDER,
            lambda d: remote(
                qsend.at[zpeer(d), :, lo:hi],
                qrecv.at[mz, :, lo:hi],
                z_send.at[k, d],
                z_recv.at[k, d],
                zdev(d),
            ),
        )
        qrecv[mz, :, lo:hi] = qsend[mz, :, lo:hi]
        return copies

    def q_sum(lo, hi):
        total = qrecv[0, :, lo:hi].astype(F32)
        for z in range(1, NZ):
            total = total + qrecv[z, :, lo:hi].astype(F32)
        return total.astype(BF)

    arrived(c_n)
    arrived(c_wa)
    q_chunk(0, wq, 0, 256, 0)
    c_qa = q_exchange(1, 0, 256)
    arrived(c_wb)
    q_chunk(1, wq, 256, 512, 256)
    c_qb = q_exchange(2, 256, 512)
    arrived(c_wk)
    arrived(c_wv)
    q_chunk(2, wk, 0, 128, 512)
    q_chunk(2, wv, 0, 128, 640)
    c_qc = q_exchange(3, 512, 768)
    own_cols = pl.ds(pl.multiple_of(mt * 512, 512), 512)
    c_tok = exchange(
        Z_ORDER,
        lambda d: remote(
            tokens.at[:, own_cols],
            tok_all.at[mz, :, own_cols],
            z_send.at[4, d],
            z_recv.at[4, d],
            zdev(d),
        ),
    )
    c_wd = exchange(
        Z_ORDER,
        lambda d: remote(
            wd_all.at[mz], wd_all.at[mz], z_send.at[5, d], z_recv.at[5, d], zdev(d)
        ),
    )
    for copy in kv_copies:
        copy.wait()
    arrived(c_qa)
    total_a = q_sum(0, 256)
    arrived(c_qb)
    total_b = q_sum(256, 512)

    q_rows = jnp.zeros((64, 128), F32)
    for h in range(4):
        part = (total_a, total_b)[h // 2][:, 128 * (h % 2) : 128 * (h % 2 + 1)]
        spread = one_if(iota((64, 16), 0) == 4 * iota((64, 16), 1) + h).astype(BF)
        q_rows = q_rows + dot(spread, part)
    q64[...] = q_rows
    first = iota((8, 128), 0) < 4
    for p in range(8):
        q8 = q64[8 * p : 8 * p + 8]
        qa = jnp.where(first, q8, 0.0).astype(BF)
        qb = jnp.where(first, 0.0, q8).astype(BF)
        scores[8 * p : 8 * p + 8] = dot_nt(qa, keys[2 * p]) + dot_nt(qb, keys[2 * p + 1])

    c_ftok = []
    for copy, d in reversed(list(zip(c_tok, Z_ORDER))):
        copy.wait_recv()
        block = tok_all.at[zsource(d), :, own_cols]
        c_ftok += exchange(
            T_ORDER,
            lambda e: remote(block, block, ft_send.at[d, e], ft_recv.at[d, e], tdev(e)),
        )

    row = iota((64, 1), 0)
    head = jnp.bitwise_and(row, 3)
    seq = lax.shift_right_logical(row, 2)
    bias_col = jnp.zeros((64, 1), F32)
    for h in range(4):
        bias_col = jnp.where(head == h, bias[h], bias_col)
    len_col = jnp.zeros((64, 1), jnp.int32)
    for s in range(16):
        len_col = jnp.where(seq == s, lengths[s], len_col)
    after = one_if(iota((128, 128), 0) > iota((128, 128), 1)).astype(BF)
    carry = jnp.zeros((64, 1), F32)
    for b in reversed(range(8)):
        cols = slice(128 * b, 128 * (b + 1))
        zz = scores[:, cols] * (128 ** (-0.5)) + bias_col
        inside = (iota((64, 128), 1) + 128 * b) < len_col
        soft = jnp.log1p(jnp.exp(-jnp.abs(zz)))
        keep = jnp.where(inside, jnp.minimum(-zz, 0.0) - soft, 0.0)
        take = jnp.minimum(zz, 0.0) - soft
        k1 = keep.astype(BF)
        r1 = keep - k1.astype(F32)
        k2 = r1.astype(BF)
        k3 = (r1 - k2.astype(F32)).astype(BF)
        between = dot(k1, after) + dot(k2, after) + dot(k3, after) + carry
        carry = between[:, 0:1] + keep[:, 0:1]
        scores[:, cols] = jnp.where(inside, jnp.exp(take + between), 0.0)

    for p in range(8):
        w8 = scores[8 * p : 8 * p + 8].astype(BF)
        att64[8 * p : 8 * p + 8] = jnp.where(
            first, dot(w8, values[2 * p]), dot(w8, values[2 * p + 1])
        )
    att_rows = att64[...].astype(BF)
    for h in range(4):
        pick = one_if(iota((16, 64), 1) == 4 * iota((16, 64), 0) + h).astype(BF)
        att_all[mz, :, 128 * h : 128 * (h + 1)] = dot(pick, att_rows).astype(BF)

    c_a = exchange(
        Z_ORDER,
        lambda d: remote(
            att_all.at[mz], att_all.at[mz], z_send.at[6, d], z_recv.at[6, d], zdev(d)
        ),
    )
    arrived(c_qc)
    out[:, 512:768] = q_sum(512, 768)
    arrived(c_wd)
    slot_of_row = 16 * mz + 2 * lax.shift_right_logical(iota((128, 128), 0), 4)
    slot_of_row = slot_of_row + jnp.bitwise_and(iota((128, 128), 0), 1)
    spread = one_if(slot_of_row == iota((128, 128), 1)).astype(BF)
    row_z = jnp.bitwise_and(lax.shift_right_logical(iota((128, 128), 0), 1), 7)
    own_z = row_z == lax.shift_right_logical(iota((128, 128), 1), 4)
    wd = wd_all[...].reshape(128, 128)
    wd_hi = wd.astype(BF)
    wd_lo = (wd - wd_hi.astype(F32)).astype(BF)
    filled = one_if(wd > 0.0).astype(BF)
    dispatch = jnp.where(own_z, dot_nt(spread, filled), 0.0).astype(BF)
    row_z_t = jnp.bitwise_and(lax.shift_right_logical(iota((128, 128), 1), 1), 7)
    own_z_t = row_z_t == lax.shift_right_logical(iota((128, 128), 0), 4)
    comb_hi = jnp.where(own_z_t, dot_nt(wd_hi, spread), 0.0).astype(BF)
    comb_lo = jnp.where(own_z_t, dot_nt(wd_lo, spread), 0.0).astype(BF)
    arrived(c_wo)
    arrived(c_a)
    po_send[...] = (
        dot_nt(att_all[...].reshape(128, 512), wo[...].reshape(256, 512))
        .astype(BF)
        .reshape(NT, 32, 256)
    )
    c_po = exchange(
        T_ORDER,
        lambda d: remote(
            po_send.at[tpeer(d)], po_recv.at[mt], t_send.at[0, d], t_recv.at[0, d], tdev(d)
        ),
    )
    po_recv[mt] = po_send[mt]
    arrived(c_po)
    part = po_recv[0].astype(F32)
    for t in range(1, NT):
        part = part + po_recv[t].astype(F32)
    mixed[mt, mz] = part.astype(BF)

    own_block = mixed.at[mt, mz]
    c_mx = exchange(
        Z_ORDER,
        lambda d: remote(own_block, own_block, z_send.at[7, d], z_recv.at[7, d], zdev(d)),
    )
    c_fm = exchange(
        T_ORDER,
        lambda e: remote(own_block, own_block, fm_send.at[0, e], fm_recv.at[0, e], tdev(e)),
    )
    for copy, d in reversed(list(zip(c_mx, Z_ORDER))):
        copy.wait_recv()
        block = mixed.at[mt, zsource(d)]
        c_fm += exchange(
            T_ORDER,
            lambda e: remote(block, block, fm_send.at[d, e], fm_recv.at[d, e], tdev(e)),
        )
    for copy in c_ftok:
        copy.wait_recv()
    for copy in c_fm:
        copy.wait_recv()
    for z in range(NZ):
        pieces = []
        square = jnp.zeros((16, 1), F32)
        for s in range(NZ):
            cols = slice(256 * s, 256 * (s + 1))
            piece = tok_all[z, :, cols].astype(F32) + mixed[
                z // 2, s, 16 * (z % 2) : 16 * (z % 2) + 16
            ].astype(F32)
            square = square + jnp.sum(piece * piece, axis=-1, keepdims=True)
            pieces.append(piece)
        scale = lax.rsqrt(square * (1.0 / 2048) + norm_eps)
        for s in range(NZ):
            cols = slice(256 * s, 256 * (s + 1))
            xs[z, :, cols] = (pieces[s] * scale * ffn_gain[:, cols]).astype(BF)

    for b in range(4):
        cols = slice(512 * b, 512 * (b + 1))
        row_send[:, :, cols] = (
            dot(dispatch, xs[:, :, cols].reshape(128, 512)).astype(BF).reshape(NJ, 16, 512)
        )
    c_row = exchange(
        J_ORDER,
        lambda d: remote(
            row_send.at[jpeer(d)], row_recv.at[mj], j_send.at[7, d], j_recv.at[7, d], jdev(d)
        ),
    )
    row_recv[mj] = row_send[mj]

    for copy in locals_:
        copy.wait()
    arrived(c_dg)
    arrived(c_du)
    x_own = xs[:, :, own_cols].reshape(128, 512)
    for t in range(NT):
        cols = slice(256 * t, 256 * (t + 1))
        pd_send[t, :, 0:256] = dot(x_own, dgate[:, cols]).astype(BF)
        pd_send[t, :, 256:512] = dot(x_own, dup[:, cols]).astype(BF)
    c_pd = exchange(
        T_ORDER,
        lambda d: remote(
            pd_send.at[tpeer(d)], pd_recv.at[mt], t_send.at[1, d], t_recv.at[1, d], tdev(d)
        ),
    )
    pd_recv[mt] = pd_send[mt]
    weighted = jnp.zeros((128, 128), F32)
    for r in range(16):
        weighted = weighted + (
            xs[:, :, 128 * r : 128 * (r + 1)].reshape(128, 128).astype(F32)
            * branch_gate[r : r + 1, :].astype(F32)
        )
    branch = jax.nn.sigmoid(jnp.sum(weighted, axis=-1, keepdims=True))
    arrived(c_pd)
    pre = pd_recv[0].astype(F32)
    for t in range(1, NT):
        pre = pre + pd_recv[t].astype(F32)
    gate_d = pre[:, 0:256]
    hid[mt] = (gate_d * jax.nn.sigmoid(gate_d) * pre[:, 256:512]).astype(BF)
    c_h = exchange(
        T_ORDER,
        lambda d: remote(hid.at[mt], hid.at[mt], t_send.at[2, d], t_recv.at[2, d], tdev(d)),
    )

    arrived(c_row)
    rows = row_recv[...].reshape(128, 2048)
    gate_c = jnp.minimum(dot(rows, egate[...]), clamp_limit)
    up_c = jnp.clip(dot(rows, eup[...]), -clamp_limit, clamp_limit)
    unit = ((up_c + 1.0) * gate_c * jax.nn.sigmoid(swish_alpha * gate_c)).astype(BF)
    for t in range(NT):
        pe_send[t] = dot(unit, edown[:, 512 * t : 512 * (t + 1)]).astype(BF)
    c_pe = exchange(
        T_ORDER,
        lambda d: remote(
            pe_send.at[tpeer(d)], pe_recv.at[mt], t_send.at[3, d], t_recv.at[3, d], tdev(d)
        ),
    )
    pe_recv[mt] = pe_send[mt]

    arrived(c_h)
    arrived(c_dd)
    down = dot(hid[0], ddown[0:256])
    for t in range(1, NT):
        down = down + dot(hid[t], ddown[256 * t : 256 * (t + 1)])
    dense_part[...] = down * branch

    arrived(c_pe)
    total_e = pe_recv[0].astype(F32)
    for t in range(1, NT):
        total_e = total_e + pe_recv[t].astype(F32)
    er[...] = total_e.astype(BF).reshape(NJ, 16, 512)
    c_er = exchange(
        J_ORDER,
        lambda d: remote(
            er.at[jpeer(d)], er_recv.at[mj], j_send.at[8, d], j_recv.at[8, d], jdev(d)
        ),
    )
    er_recv[mj] = er[mj]
    arrived(c_er)
    back = er_recv[...].reshape(128, 512)
    fin_send[...] = (
        (dot(comb_hi, back) + dot(comb_lo, back) + dense_part[...]).astype(BF).reshape(NZ, 16, 512)
    )
    c_f = exchange(
        Z_ORDER,
        lambda d: remote(
            fin_send.at[zpeer(d)], fin_recv.at[mz], z_send.at[8, d], z_recv.at[8, d], zdev(d)
        ),
    )
    fin_recv[mz] = fin_send[mz]
    quarter = lax.div(mz, 2)
    own_rows = pl.ds(pl.multiple_of(lax.rem(mz, 2) * 16, 16), 16)
    final = tokens[:, own_cols].astype(F32) + jnp.concatenate(
        [mixed[quarter, 2 * mt, own_rows], mixed[quarter, 2 * mt + 1, own_rows]], axis=1
    ).astype(F32)
    arrived(c_f)
    for z in range(NZ):
        final = final + fin_recv[z].astype(F32)
    out[:, 0:512] = final.astype(BF)

    for copy in started:
        copy.wait_send()


def split_kernel(both, layer_out, new_keys, new_values):
    layer_out[...] = both[:, 0:512]
    new_keys[...] = both[:, 512:640]
    new_values[...] = both[:, 640:768]


def body(
    tokens,
    attn_gain,
    query_weight,
    key_weight,
    value_weight,
    break_bias,
    cache_keys,
    cache_values,
    lengths,
    out_weight,
    ffn_gain,
    branch_gate,
    dense_gate,
    dense_up,
    dense_down,
    route_ids,
    route_weights,
    expert_gate,
    expert_up,
    expert_down,
):
    vm = pl.BlockSpec(memory_space=pltpu.VMEM)
    sm = pl.BlockSpec(memory_space=pltpu.SMEM)
    hbm = pl.BlockSpec(memory_space=pl.ANY)
    V = pltpu.VMEM
    D = pltpu.SemaphoreType.DMA
    both = pl.pallas_call(
        kernel,
        name="layer",
        out_shape=jax.ShapeDtypeStruct((16, 768), BF),
        in_specs=[hbm] * 5 + [sm, hbm, hbm, sm] + [hbm] * 11,
        out_specs=vm,
        scratch_shapes=[
            V((16, 2048), BF),
            V((1, 2048), F32),
            V((32, 512), BF),
            V((32, 128), BF),
            V((32, 128), BF),
            V((32, 512), BF),
            V((1, 2048), F32),
            V((16, 128), BF),
            V((4, 16), jnp.int32),
            V((4, 16), F32),
            V((16, 1024, 128), BF),
            V((16, 1024, 128), BF),
            V((2048, 256), BF),
            V((2048, 256), BF),
            V((256, 2048), BF),
            V((512, 1024), BF),
            V((512, 1024), BF),
            V((1024, 512), BF),
            V((NJ, 32, 512), BF),
            V((NJ, 32, 128), BF),
            V((NJ, 32, 128), BF),
            V((NJ, 32, 512), BF),
            V((NZ, 16, 256), BF),
            V((NZ, 16, 256), BF),
            V((NZ, 16, 768), BF),
            V((NZ, 16, 768), BF),
            V((64, 1024), F32),
            V((64, 128), F32),
            V((64, 128), F32),
            V((NZ, 16, 512), BF),
            V((NZ, 16, 128), F32),
            V((NZ, 16, 2048), BF),
            V((NT, 32, 256), BF),
            V((NT, 32, 256), BF),
            V((NT, NZ, 32, 256), BF),
            V((NZ, 16, 2048), BF),
            V((NJ, 16, 2048), BF),
            V((NJ, 16, 2048), BF),
            V((NT, 128, 512), BF),
            V((NT, 128, 512), BF),
            V((NT, 128, 256), BF),
            V((NT, 128, 512), BF),
            V((NT, 128, 512), BF),
            V((NJ, 16, 512), BF),
            V((NJ, 16, 512), BF),
            V((128, 512), F32),
            V((NZ, 16, 512), BF),
            V((NZ, 16, 512), BF),
            D((10,)),
            D((6,)),
            D((16,)),
            D((9, NZ)),
            D((9, NZ)),
            D((10, NJ)),
            D((10, NJ)),
            D((4, NT)),
            D((4, NT)),
            D((NZ, NT)),
            D((NZ, NT)),
            D((NZ, NT)),
            D((NZ, NT)),
        ],
        compiler_params=pltpu.CompilerParams(
            collective_id=0,
            has_side_effects=True,
            vmem_limit_bytes=60 * 1024 * 1024,
        ),
    )(
        tokens,
        attn_gain.reshape(1, -1),
        query_weight,
        key_weight,
        value_weight,
        break_bias,
        cache_keys,
        cache_values,
        lengths,
        out_weight.T,
        ffn_gain.reshape(1, -1),
        branch_gate.reshape(16, 128),
        dense_gate,
        dense_up,
        dense_down,
        route_ids.T,
        route_weights.T,
        expert_gate,
        expert_up,
        expert_down,
    )
    return tuple(
        pl.pallas_call(
            split_kernel,
            name="split",
            out_shape=(
                jax.ShapeDtypeStruct((16, 512), BF),
                jax.ShapeDtypeStruct((16, 128), BF),
                jax.ShapeDtypeStruct((16, 128), BF),
            ),
            in_specs=[vm],
            out_specs=(vm, vm, vm),
        )(both)
    )


def solution(mesh):
    split = Mesh(mesh.devices.reshape(NZ, NX, NC, NT), ("z", "x", "c", "tp"))
    return jax.shard_map(
        body,
        mesh=split,
        in_specs=(
            P(EP, None),
            P(),
            P(EP, "tp"),
            P(EP, "tp"),
            P(EP, "tp"),
            P("tp"),
            P(EP, "tp", None, None),
            P(EP, "tp", None, None),
            P(EP),
            P("tp", EP),
            P(),
            P(),
            P("tp", EP),
            P("tp", EP),
            P(EP, "tp"),
            P(EP, None),
            P(EP, None),
            P(EP, None, "tp"),
            P(EP, None, "tp"),
            P(EP, "tp", None),
        ),
        out_specs=(P(EP, "tp"), P(EP, "tp"), P(EP, "tp")),
        check_vma=False,
    )
```

```python
import functools

import jax
import jax.numpy as jnp
from jax import lax
from jax.experimental import pallas as pl
from jax.experimental.pallas import tpu as pltpu
from jax.sharding import Mesh
from jax.sharding import PartitionSpec as P

EP = ("z", "x", "c")
NZ, NX, NC, NT = 8, 4, 2, 4
NJ = NX * NC

norm_eps = 1e-05
clamp_limit = 7.0
swish_alpha = 1.702

BF = jnp.bfloat16
F32 = jnp.float32
MESH_IDS = pl.DeviceIdType.MESH


def dot(a, b):
    return jnp.dot(a, b, preferred_element_type=F32)


def dot_nt(a, b):
    return lax.dot_general(a, b, (((1,), (1,)), ((), ())), preferred_element_type=F32)


def iota(shape, dim):
    return lax.broadcasted_iota(jnp.int32, shape, dim)


def one_if(mask):
    return jnp.where(mask, 1.0, 0.0)


Z_ORDER = (4, 3, 5, 2, 6, 1, 7)
J_ORDER = (4, 3, 5, 2, 6, 1, 7)
T_ORDER = (2, 1, 3)


def kernel(
    tokens_in,
    attn_gain_in,
    wq_hbm,
    wk_hbm,
    wv_hbm,
    bias,
    keys_hbm,
    values_hbm,
    lengths,
    wo_hbm,
    ffn_gain_in,
    branch_gate_in,
    dgate_hbm,
    dup_hbm,
    ddown_hbm,
    route_ids_in,
    route_weights_in,
    egate_hbm,
    eup_hbm,
    edown_hbm,
    out,
    tokens,
    attn_gain,
    wq_in,
    wk_in,
    wv_in,
    wo_in,
    ffn_gain,
    branch_gate,
    route_ids,
    route_weights,
    keys,
    values,
    egate,
    eup,
    edown,
    dgate,
    dup,
    ddown,
    wq,
    wk,
    wv,
    wo,
    nsend,
    nslab,
    qsend,
    qrecv,
    scores,
    q64,
    att64,
    att_all,
    wd_all,
    tok_all,
    po_send,
    po_recv,
    mixed,
    xs,
    row_send,
    row_recv,
    pd_send,
    pd_recv,
    hid,
    pe_send,
    pe_recv,
    er,
    er_recv,
    dense_part,
    fin_send,
    fin_recv,
    in_sem,
    local_sem,
    kv_sem,
    z_send,
    z_recv,
    j_send,
    j_recv,
    t_send,
    t_recv,
    ft_send,
    ft_recv,
    fm_send,
    fm_recv,
    p_send,
    p_recv,
):
    mz = lax.axis_index("z")
    mxx = lax.axis_index("x")
    mc = lax.axis_index("c")
    mt = lax.axis_index("tp")
    mj = mxx * NC + mc

    def zpeer(d):
        return lax.rem(mz + d, NZ)

    def zsource(d):
        return lax.rem(mz + NZ - d, NZ)

    def jpeer(d):
        return lax.rem(mj + d, NJ)

    def tpeer(d):
        return lax.rem(mt + d, NT)

    def zdev(d):
        return {"z": zpeer(d)}

    def jdev(d):
        j = jpeer(d)
        return {"x": lax.div(j, NC), "c": lax.rem(j, NC)}

    def tdev(d):
        return {"tp": tpeer(d)}

    def remote(src, dst, ssem, rsem, dev):
        return pltpu.make_async_remote_copy(
            src_ref=src,
            dst_ref=dst,
            send_sem=ssem,
            recv_sem=rsem,
            device_id=dev,
            device_id_type=MESH_IDS,
        )

    started = []

    def exchange(order, make):
        copies = [make(d) for d in order]
        for copy in copies:
            copy.start()
        started.extend(copies)
        return copies

    def arrived(copies):
        for copy in reversed(copies):
            copy.wait_recv()

    barrier = pltpu.get_barrier_semaphore()
    for d in Z_ORDER:
        pl.semaphore_signal(barrier, inc=1, device_id=zdev(d), device_id_type=MESH_IDS)
    for d in J_ORDER:
        pl.semaphore_signal(barrier, inc=1, device_id=jdev(d), device_id_type=MESH_IDS)
    for d in T_ORDER:
        pl.semaphore_signal(barrier, inc=1, device_id=tdev(d), device_id_type=MESH_IDS)

    inputs = [
        pltpu.make_async_copy(src, dst, in_sem.at[k])
        for k, (src, dst) in enumerate(
            (
                (tokens_in, tokens),
                (attn_gain_in, attn_gain),
                (wq_hbm, wq_in),
                (wk_hbm, wk_in),
                (wv_hbm, wv_in),
                (route_ids_in, route_ids),
                (route_weights_in, route_weights),
                (wo_hbm, wo_in),
                (ffn_gain_in, ffn_gain),
                (branch_gate_in, branch_gate),
            )
        )
    ]
    for copy in inputs:
        copy.start()
    kv_copies = []
    for s in range(0, 16, 2):
        kv_copies.append(
            pltpu.make_async_copy(
                keys_hbm.at[pl.ds(s, 2), 0], keys.at[pl.ds(s, 2)], kv_sem.at[s]
            )
        )
    for s in range(0, 16, 2):
        kv_copies.append(
            pltpu.make_async_copy(
                values_hbm.at[pl.ds(s, 2), 0], values.at[pl.ds(s, 2)], kv_sem.at[s + 1]
            )
        )
    for copy in kv_copies:
        copy.start()
    dense_col = pl.ds(pl.multiple_of(mj * 128, 128), 128)
    locals_ = [
        pltpu.make_async_copy(dgate_hbm, dgate.at[:, dense_col], local_sem.at[0]),
        pltpu.make_async_copy(dup_hbm, dup.at[:, dense_col], local_sem.at[1]),
        pltpu.make_async_copy(ddown_hbm, ddown.at[dense_col], local_sem.at[2]),
        pltpu.make_async_copy(egate_hbm.at[0], egate, local_sem.at[3]),
        pltpu.make_async_copy(eup_hbm.at[0], eup, local_sem.at[4]),
        pltpu.make_async_copy(edown_hbm.at[0], edown, local_sem.at[5]),
    ]
    for copy in locals_:
        copy.start()

    for copy in inputs[0:2]:
        copy.wait()
    tok = tokens[...].astype(F32)
    normed = (
        tok * lax.rsqrt(jnp.mean(tok * tok, axis=-1, keepdims=True) + norm_eps) * attn_gain[...]
    ).astype(BF)
    for z in range(NZ):
        nsend[z] = normed[:, 256 * z : 256 * (z + 1)]
    for copy in inputs[2:]:
        copy.wait()

    pl.semaphore_wait(barrier, NJ + NZ + NT - 3)

    def chunk_of(src, dst, k, lo, hi):
        return exchange(
            J_ORDER,
            lambda d: remote(
                src.at[:, lo:hi],
                dst.at[mj, :, lo:hi],
                j_send.at[k, d],
                j_recv.at[k, d],
                jdev(d),
            ),
        )

    c_wa = chunk_of(wq_in, wq, 0, 0, 256)
    c_n = exchange(
        Z_ORDER,
        lambda d: remote(
            nsend.at[zpeer(d)], nslab.at[mz], z_send.at[0, d], z_recv.at[0, d], zdev(d)
        ),
    )
    own_cols = pl.ds(pl.multiple_of(mt * 512, 512), 512)
    c_tok = exchange(
        Z_ORDER,
        lambda d: remote(
            tokens.at[:, own_cols],
            tok_all.at[mz, :, own_cols],
            z_send.at[4, d],
            z_recv.at[4, d],
            zdev(d),
        ),
    )
    c_wb = chunk_of(wq_in, wq, 1, 256, 512)
    c_wk = chunk_of(wk_in, wk, 2, 0, 128)
    c_wv = chunk_of(wv_in, wv, 9, 0, 128)
    c_wo = exchange(
        J_ORDER, lambda d: remote(wo_in, wo.at[mj], j_send.at[3, d], j_recv.at[3, d], jdev(d))
    )
    dense = (
        (dgate_hbm, lambda j: dgate.at[:, pl.ds(pl.multiple_of(j * 128, 128), 128)]),
        (dup_hbm, lambda j: dup.at[:, pl.ds(pl.multiple_of(j * 128, 128), 128)]),
        (ddown_hbm, lambda j: ddown.at[pl.ds(pl.multiple_of(j * 128, 128), 128)]),
    )
    c_dx = [
        exchange(
            (4, 2, 6),
            lambda d: remote(src, part(mj), j_send.at[4 + k, d], j_recv.at[4 + k, d], jdev(d)),
        )
        for k, (src, part) in enumerate(dense)
    ]
    partner = {"c": 1 - mc}
    c_dp = [
        exchange(
            (0,),
            lambda d: remote(src, part(mj), p_send.at[k, d], p_recv.at[k, d], partner),
        )
        for k, (src, part) in enumerate(dense)
    ]
    wq[mj] = wq_in[...]
    wk[mj] = wk_in[...]
    wv[mj] = wv_in[...]
    wo[mj] = wo_in[...]
    nslab[mz] = nsend[mz]
    tok_all[mz] = tokens[...]

    row_expert = lax.shift_right_logical(iota((128, 16), 0), 1)
    named = jnp.zeros((128, 16), F32)
    weighed = jnp.zeros((128, 16), F32)
    for k in range(4):
        hit = route_ids[k : k + 1, :] == row_expert
        named = named + one_if(hit)
        weighed = weighed + jnp.where(hit, route_weights[k : k + 1, :], 0.0)
    earlier = one_if(iota((16, 16), 0) < iota((16, 16), 1)).astype(BF)
    rank = dot(named.astype(BF), earlier)
    row_rank = jnp.bitwise_and(iota((128, 16), 0), 1).astype(F32)
    slots = jnp.where(rank == row_rank, weighed, 0.0)
    wd_all[mz] = jnp.concatenate([slots, jnp.zeros((128, 112), F32)], axis=1).T[0:16]

    def q_chunk(k, weight, lo, hi, at):
        width = hi - lo
        cols = slice(at, at + width)
        qsend[:, :, cols] = (
            dot(nslab[...].reshape(128, 256), weight[:, :, lo:hi].reshape(256, width))
            .astype(BF)
            .reshape(NZ, 16, width)
        )

    def q_exchange(k, lo, hi):
        copies = exchange(
            Z_ORDER,
            lambda d: remote(
                qsend.at[zpeer(d), :, lo:hi],
                qrecv.at[mz, :, lo:hi],
                z_send.at[k, d],
                z_recv.at[k, d],
                zdev(d),
            ),
        )
        qrecv[mz, :, lo:hi] = qsend[mz, :, lo:hi]
        return copies

    def q_sum(lo, hi):
        total = qrecv[0, :, lo:hi].astype(F32)
        for z in range(1, NZ):
            total = total + qrecv[z, :, lo:hi].astype(F32)
        return total.astype(BF)

    arrived(c_n)
    arrived(c_wa)
    q_chunk(0, wq, 0, 256, 0)
    c_qa = q_exchange(1, 0, 256)
    arrived(c_wb)
    q_chunk(1, wq, 256, 512, 256)
    c_qb = q_exchange(2, 256, 512)
    arrived(c_wk)
    arrived(c_wv)
    q_chunk(2, wk, 0, 128, 512)
    q_chunk(2, wv, 0, 128, 640)
    c_qc = q_exchange(3, 512, 768)
    c_wd = exchange(
        Z_ORDER,
        lambda d: remote(
            wd_all.at[mz], wd_all.at[mz], z_send.at[5, d], z_recv.at[5, d], zdev(d)
        ),
    )
    c_ftok = []
    for copy, d in reversed(list(zip(c_tok, Z_ORDER))):
        copy.wait_recv()
        block = tok_all.at[zsource(d), :, own_cols]
        c_ftok += exchange(
            T_ORDER,
            lambda e: remote(block, block, ft_send.at[d, e], ft_recv.at[d, e], tdev(e)),
        )

    for copy in kv_copies:
        copy.wait()
    arrived(c_qa)
    total_a = q_sum(0, 256)
    arrived(c_qb)
    total_b = q_sum(256, 512)

    q_rows = jnp.zeros((64, 128), F32)
    for h in range(4):
        part = (total_a, total_b)[h // 2][:, 128 * (h % 2) : 128 * (h % 2 + 1)]
        spread = one_if(iota((64, 16), 0) == 4 * iota((64, 16), 1) + h).astype(BF)
        q_rows = q_rows + dot(spread, part)
    q64[...] = q_rows
    first = iota((8, 128), 0) < 4
    for p in range(8):
        q8 = q64[8 * p : 8 * p + 8]
        qa = jnp.where(first, q8, 0.0).astype(BF)
        qb = jnp.where(first, 0.0, q8).astype(BF)
        scores[8 * p : 8 * p + 8] = dot_nt(qa, keys[2 * p]) + dot_nt(qb, keys[2 * p + 1])

    row = iota((64, 1), 0)
    head = jnp.bitwise_and(row, 3)
    seq = lax.shift_right_logical(row, 2)
    bias_col = jnp.zeros((64, 1), F32)
    for h in range(4):
        bias_col = jnp.where(head == h, bias[h], bias_col)
    len_col = jnp.zeros((64, 1), jnp.int32)
    for s in range(16):
        len_col = jnp.where(seq == s, lengths[s], len_col)
    after = one_if(iota((128, 128), 0) > iota((128, 128), 1)).astype(BF)
    carry = jnp.zeros((64, 1), F32)
    for b in reversed(range(8)):
        cols = slice(128 * b, 128 * (b + 1))
        zz = scores[:, cols] * (128 ** (-0.5)) + bias_col
        inside = (iota((64, 128), 1) + 128 * b) < len_col
        soft = jnp.log1p(jnp.exp(-jnp.abs(zz)))
        keep = jnp.where(inside, jnp.minimum(-zz, 0.0) - soft, 0.0)
        take = jnp.minimum(zz, 0.0) - soft
        k1 = keep.astype(BF)
        r1 = keep - k1.astype(F32)
        k2 = r1.astype(BF)
        k3 = (r1 - k2.astype(F32)).astype(BF)
        between = dot(k1, after) + dot(k2, after) + dot(k3, after) + carry
        carry = between[:, 0:1] + keep[:, 0:1]
        scores[:, cols] = jnp.where(inside, jnp.exp(take + between), 0.0)

    for p in range(8):
        w8 = scores[8 * p : 8 * p + 8].astype(BF)
        att64[8 * p : 8 * p + 8] = jnp.where(
            first, dot(w8, values[2 * p]), dot(w8, values[2 * p + 1])
        )
    att_rows = att64[...].astype(BF)
    for h in range(4):
        pick = one_if(iota((16, 64), 1) == 4 * iota((16, 64), 0) + h).astype(BF)
        att_all[mz, :, 128 * h : 128 * (h + 1)] = dot(pick, att_rows).astype(BF)

    c_a = exchange(
        Z_ORDER,
        lambda d: remote(
            att_all.at[mz], att_all.at[mz], z_send.at[6, d], z_recv.at[6, d], zdev(d)
        ),
    )
    arrived(c_qc)
    out[:, 512:768] = q_sum(512, 768)
    arrived(c_wd)
    slot_of_row = 16 * mz + 2 * lax.shift_right_logical(iota((128, 128), 0), 4)
    slot_of_row = slot_of_row + jnp.bitwise_and(iota((128, 128), 0), 1)
    spread = one_if(slot_of_row == iota((128, 128), 1)).astype(BF)
    row_z = jnp.bitwise_and(lax.shift_right_logical(iota((128, 128), 0), 1), 7)
    own_z = row_z == lax.shift_right_logical(iota((128, 128), 1), 4)
    wd = wd_all[...].reshape(128, 128)
    wd_hi = wd.astype(BF)
    wd_lo = (wd - wd_hi.astype(F32)).astype(BF)
    filled = one_if(wd > 0.0).astype(BF)
    dispatch = jnp.where(own_z, dot_nt(spread, filled), 0.0).astype(BF)
    row_z_t = jnp.bitwise_and(lax.shift_right_logical(iota((128, 128), 1), 1), 7)
    own_z_t = row_z_t == lax.shift_right_logical(iota((128, 128), 0), 4)
    comb_hi = jnp.where(own_z_t, dot_nt(wd_hi, spread), 0.0).astype(BF)
    comb_lo = jnp.where(own_z_t, dot_nt(wd_lo, spread), 0.0).astype(BF)
    arrived(c_wo)
    arrived(c_a)
    po_send[...] = (
        dot_nt(att_all[...].reshape(128, 512), wo[...].reshape(256, 512))
        .astype(BF)
        .reshape(NT, 32, 256)
    )
    c_po = exchange(
        T_ORDER,
        lambda d: remote(
            po_send.at[tpeer(d)], po_recv.at[mt], t_send.at[0, d], t_recv.at[0, d], tdev(d)
        ),
    )
    po_recv[mt] = po_send[mt]
    arrived(c_po)
    part = po_recv[0].astype(F32)
    for t in range(1, NT):
        part = part + po_recv[t].astype(F32)
    mixed[mt, mz] = part.astype(BF)

    own_block = mixed.at[mt, mz]
    c_mx = exchange(
        Z_ORDER,
        lambda d: remote(own_block, own_block, z_send.at[7, d], z_recv.at[7, d], zdev(d)),
    )
    c_fm = exchange(
        T_ORDER,
        lambda e: remote(own_block, own_block, fm_send.at[0, e], fm_recv.at[0, e], tdev(e)),
    )
    for k, (src, part) in enumerate(dense):
        arrived(c_dx[k])
        c_dp[k] += exchange(
            (2, 4, 6),
            lambda d: remote(
                part(lax.rem(mj + NJ - d, NJ)),
                part(lax.rem(mj + NJ - d, NJ)),
                p_send.at[k, d // 2],
                p_recv.at[k, d // 2],
                partner,
            ),
        )
    for copy, d in reversed(list(zip(c_mx, Z_ORDER))):
        copy.wait_recv()
        block = mixed.at[mt, zsource(d)]
        c_fm += exchange(
            T_ORDER,
            lambda e: remote(block, block, fm_send.at[d, e], fm_recv.at[d, e], tdev(e)),
        )
    for copy in c_ftok:
        copy.wait_recv()
    for copy in c_fm:
        copy.wait_recv()
    for z in range(NZ):
        pieces = []
        square = jnp.zeros((16, 1), F32)
        for s in range(NZ):
            cols = slice(256 * s, 256 * (s + 1))
            piece = tok_all[z, :, cols].astype(F32) + mixed[
                z // 2, s, 16 * (z % 2) : 16 * (z % 2) + 16
            ].astype(F32)
            square = square + jnp.sum(piece * piece, axis=-1, keepdims=True)
            pieces.append(piece)
        scale = lax.rsqrt(square * (1.0 / 2048) + norm_eps)
        for s in range(NZ):
            cols = slice(256 * s, 256 * (s + 1))
            xs[z, :, cols] = (pieces[s] * scale * ffn_gain[:, cols]).astype(BF)

    for b in range(4):
        cols = slice(512 * b, 512 * (b + 1))
        row_send[:, :, cols] = (
            dot(dispatch, xs[:, :, cols].reshape(128, 512)).astype(BF).reshape(NJ, 16, 512)
        )
    c_row = exchange(
        J_ORDER,
        lambda d: remote(
            row_send.at[jpeer(d)], row_recv.at[mj], j_send.at[7, d], j_recv.at[7, d], jdev(d)
        ),
    )
    row_recv[mj] = row_send[mj]

    for copy in locals_:
        copy.wait()
    arrived(c_dp[0])
    arrived(c_dp[1])
    x_own = xs[:, :, own_cols].reshape(128, 512)
    for t in range(NT):
        cols = slice(256 * t, 256 * (t + 1))
        pd_send[t, :, 0:256] = dot(x_own, dgate[:, cols]).astype(BF)
        pd_send[t, :, 256:512] = dot(x_own, dup[:, cols]).astype(BF)
    c_pd = exchange(
        T_ORDER,
        lambda d: remote(
            pd_send.at[tpeer(d)], pd_recv.at[mt], t_send.at[1, d], t_recv.at[1, d], tdev(d)
        ),
    )
    pd_recv[mt] = pd_send[mt]
    weighted = jnp.zeros((128, 128), F32)
    for r in range(16):
        weighted = weighted + (
            xs[:, :, 128 * r : 128 * (r + 1)].reshape(128, 128).astype(F32)
            * branch_gate[r : r + 1, :].astype(F32)
        )
    branch = jax.nn.sigmoid(jnp.sum(weighted, axis=-1, keepdims=True))
    arrived(c_pd)
    pre = pd_recv[0].astype(F32)
    for t in range(1, NT):
        pre = pre + pd_recv[t].astype(F32)
    gate_d = pre[:, 0:256]
    hid[mt] = (gate_d * jax.nn.sigmoid(gate_d) * pre[:, 256:512]).astype(BF)
    c_h = exchange(
        T_ORDER,
        lambda d: remote(hid.at[mt], hid.at[mt], t_send.at[2, d], t_recv.at[2, d], tdev(d)),
    )

    arrived(c_row)
    rows = row_recv[...].reshape(128, 2048)
    gate_c = jnp.minimum(dot(rows, egate[...]), clamp_limit)
    up_c = jnp.clip(dot(rows, eup[...]), -clamp_limit, clamp_limit)
    unit = ((up_c + 1.0) * gate_c * jax.nn.sigmoid(swish_alpha * gate_c)).astype(BF)
    for t in range(NT):
        pe_send[t] = dot(unit, edown[:, 512 * t : 512 * (t + 1)]).astype(BF)
    c_pe = exchange(
        T_ORDER,
        lambda d: remote(
            pe_send.at[tpeer(d)], pe_recv.at[mt], t_send.at[3, d], t_recv.at[3, d], tdev(d)
        ),
    )
    pe_recv[mt] = pe_send[mt]

    arrived(c_h)
    arrived(c_dp[2])
    down = dot(hid[0], ddown[0:256])
    for t in range(1, NT):
        down = down + dot(hid[t], ddown[256 * t : 256 * (t + 1)])
    dense_part[...] = down * branch

    arrived(c_pe)
    total_e = pe_recv[0].astype(F32)
    for t in range(1, NT):
        total_e = total_e + pe_recv[t].astype(F32)
    er[...] = total_e.astype(BF).reshape(NJ, 16, 512)
    c_er = exchange(
        J_ORDER,
        lambda d: remote(
            er.at[jpeer(d)], er_recv.at[mj], j_send.at[8, d], j_recv.at[8, d], jdev(d)
        ),
    )
    er_recv[mj] = er[mj]
    arrived(c_er)
    back = er_recv[...].reshape(128, 512)
    fin_send[...] = (
        (dot(comb_hi, back) + dot(comb_lo, back) + dense_part[...]).astype(BF).reshape(NZ, 16, 512)
    )
    c_f = exchange(
        Z_ORDER,
        lambda d: remote(
            fin_send.at[zpeer(d)], fin_recv.at[mz], z_send.at[8, d], z_recv.at[8, d], zdev(d)
        ),
    )
    fin_recv[mz] = fin_send[mz]
    quarter = lax.div(mz, 2)
    own_rows = pl.ds(pl.multiple_of(lax.rem(mz, 2) * 16, 16), 16)
    final = tokens[:, own_cols].astype(F32) + jnp.concatenate(
        [mixed[quarter, 2 * mt, own_rows], mixed[quarter, 2 * mt + 1, own_rows]], axis=1
    ).astype(F32)
    arrived(c_f)
    for z in range(NZ):
        final = final + fin_recv[z].astype(F32)
    out[:, 0:512] = final.astype(BF)

    for copy in started:
        copy.wait_send()


def split_kernel(both, layer_out, new_keys, new_values):
    layer_out[...] = both[:, 0:512]
    new_keys[...] = both[:, 512:640]
    new_values[...] = both[:, 640:768]


def body(
    tokens,
    attn_gain,
    query_weight,
    key_weight,
    value_weight,
    break_bias,
    cache_keys,
    cache_values,
    lengths,
    out_weight,
    ffn_gain,
    branch_gate,
    dense_gate,
    dense_up,
    dense_down,
    route_ids,
    route_weights,
    expert_gate,
    expert_up,
    expert_down,
):
    vm = pl.BlockSpec(memory_space=pltpu.VMEM)
    sm = pl.BlockSpec(memory_space=pltpu.SMEM)
    hbm = pl.BlockSpec(memory_space=pl.ANY)
    V = pltpu.VMEM
    D = pltpu.SemaphoreType.DMA
    both = pl.pallas_call(
        kernel,
        name="layer",
        out_shape=jax.ShapeDtypeStruct((16, 768), BF),
        in_specs=[hbm] * 5 + [sm, hbm, hbm, sm] + [hbm] * 11,
        out_specs=vm,
        scratch_shapes=[
            V((16, 2048), BF),
            V((1, 2048), F32),
            V((32, 512), BF),
            V((32, 128), BF),
            V((32, 128), BF),
            V((32, 512), BF),
            V((1, 2048), F32),
            V((16, 128), BF),
            V((4, 16), jnp.int32),
            V((4, 16), F32),
            V((16, 1024, 128), BF),
            V((16, 1024, 128), BF),
            V((2048, 256), BF),
            V((2048, 256), BF),
            V((256, 2048), BF),
            V((512, 1024), BF),
            V((512, 1024), BF),
            V((1024, 512), BF),
            V((NJ, 32, 512), BF),
            V((NJ, 32, 128), BF),
            V((NJ, 32, 128), BF),
            V((NJ, 32, 512), BF),
            V((NZ, 16, 256), BF),
            V((NZ, 16, 256), BF),
            V((NZ, 16, 768), BF),
            V((NZ, 16, 768), BF),
            V((64, 1024), F32),
            V((64, 128), F32),
            V((64, 128), F32),
            V((NZ, 16, 512), BF),
            V((NZ, 16, 128), F32),
            V((NZ, 16, 2048), BF),
            V((NT, 32, 256), BF),
            V((NT, 32, 256), BF),
            V((NT, NZ, 32, 256), BF),
            V((NZ, 16, 2048), BF),
            V((NJ, 16, 2048), BF),
            V((NJ, 16, 2048), BF),
            V((NT, 128, 512), BF),
            V((NT, 128, 512), BF),
            V((NT, 128, 256), BF),
            V((NT, 128, 512), BF),
            V((NT, 128, 512), BF),
            V((NJ, 16, 512), BF),
            V((NJ, 16, 512), BF),
            V((128, 512), F32),
            V((NZ, 16, 512), BF),
            V((NZ, 16, 512), BF),
            D((10,)),
            D((6,)),
            D((16,)),
            D((9, NZ)),
            D((9, NZ)),
            D((10, NJ)),
            D((10, NJ)),
            D((4, NT)),
            D((4, NT)),
            D((NZ, NT)),
            D((NZ, NT)),
            D((NZ, NT)),
            D((NZ, NT)),
            D((3, 4)),
            D((3, 4)),
        ],
        compiler_params=pltpu.CompilerParams(
            collective_id=0,
            has_side_effects=True,
            vmem_limit_bytes=60 * 1024 * 1024,
        ),
    )(
        tokens,
        attn_gain.reshape(1, -1),
        query_weight,
        key_weight,
        value_weight,
        break_bias,
        cache_keys,
        cache_values,
        lengths,
        out_weight.T,
        ffn_gain.reshape(1, -1),
        branch_gate.reshape(16, 128),
        dense_gate,
        dense_up,
        dense_down,
        route_ids.T,
        route_weights.T,
        expert_gate,
        expert_up,
        expert_down,
    )
    return tuple(
        pl.pallas_call(
            split_kernel,
            name="split",
            out_shape=(
                jax.ShapeDtypeStruct((16, 512), BF),
                jax.ShapeDtypeStruct((16, 128), BF),
                jax.ShapeDtypeStruct((16, 128), BF),
            ),
            in_specs=[vm],
            out_specs=(vm, vm, vm),
        )(both)
    )


def solution(mesh):
    split = Mesh(mesh.devices.reshape(NZ, NX, NC, NT), ("z", "x", "c", "tp"))
    return jax.shard_map(
        body,
        mesh=split,
        in_specs=(
            P(EP, None),
            P(),
            P(EP, "tp"),
            P(EP, "tp"),
            P(EP, "tp"),
            P("tp"),
            P(EP, "tp", None, None),
            P(EP, "tp", None, None),
            P(EP),
            P("tp", EP),
            P(),
            P(),
            P("tp", EP),
            P("tp", EP),
            P(EP, "tp"),
            P(EP, None),
            P(EP, None),
            P(EP, None, "tp"),
            P(EP, None, "tp"),
            P(EP, "tp", None),
        ),
        out_specs=(P(EP, "tp"), P(EP, "tp"), P(EP, "tp")),
        check_vma=False,
    )
```

```python
import functools

import jax
import jax.numpy as jnp
from jax import lax
from jax.experimental import pallas as pl
from jax.experimental.pallas import tpu as pltpu
from jax.sharding import Mesh
from jax.sharding import PartitionSpec as P

EP = ("z", "x", "c")
NZ, NX, NC, NT = 8, 4, 2, 4
NJ = NX * NC

norm_eps = 1e-05
clamp_limit = 7.0
swish_alpha = 1.702

BF = jnp.bfloat16
F32 = jnp.float32
MESH_IDS = pl.DeviceIdType.MESH


def dot(a, b):
    return jnp.dot(a, b, preferred_element_type=F32)


def dot_nt(a, b):
    return lax.dot_general(a, b, (((1,), (1,)), ((), ())), preferred_element_type=F32)


def iota(shape, dim):
    return lax.broadcasted_iota(jnp.int32, shape, dim)


def one_if(mask):
    return jnp.where(mask, 1.0, 0.0)


Z_ORDER = (4, 3, 5, 2, 6, 1, 7)
J_ORDER = (4, 3, 5, 2, 6, 1, 7)
T_ORDER = (2, 1, 3)
HALVES = ((0, 1, 2, 6), (4, 5, 3, 7))


def kernel(
    tokens_in,
    attn_gain_in,
    wq_hbm,
    wk_hbm,
    wv_hbm,
    bias_hbm,
    keys_hbm,
    values_hbm,
    lengths_hbm,
    wo_hbm,
    ffn_gain_in,
    branch_gate_in,
    dgate_hbm,
    dup_hbm,
    ddown_hbm,
    route_ids_in,
    route_weights_in,
    egate_hbm,
    eup_hbm,
    edown_hbm,
    out,
    tokens,
    attn_gain,
    wq_in,
    wk_in,
    wv_in,
    wo_in,
    ffn_gain,
    branch_gate,
    route_ids,
    route_weights,
    bias,
    lengths,
    keys,
    values,
    egate,
    eup,
    edown,
    dgate,
    dup,
    ddown,
    wq,
    wk,
    wv,
    wo,
    nsend,
    nslab,
    qsend,
    qrecv,
    scores,
    q64,
    att64,
    att_all,
    wd_all,
    tok_all,
    po_send,
    po_recv,
    mixed,
    xs,
    row_send,
    row_recv,
    pd_send,
    pd_recv,
    hid,
    pe_send,
    pe_recv,
    er,
    er_recv,
    dense_part,
    fin_send,
    fin_recv,
    in_sem,
    local_sem,
    kv_sem,
    z_send,
    z_recv,
    j_send,
    j_recv,
    t_send,
    t_recv,
    ft_send,
    ft_recv,
    fm_send,
    fm_recv,
    p_send,
    p_recv,
):
    mz = lax.axis_index("z")
    mxx = lax.axis_index("x")
    mc = lax.axis_index("c")
    mt = lax.axis_index("tp")
    mj = mxx * NC + mc

    def zpeer(d):
        return lax.rem(mz + d, NZ)

    def zsource(d):
        return lax.rem(mz + NZ - d, NZ)

    def jpeer(d):
        return lax.rem(mj + d, NJ)

    def tpeer(d):
        return lax.rem(mt + d, NT)

    def zdev(d):
        return {"z": zpeer(d)}

    def jdev(d):
        j = jpeer(d)
        return {"x": lax.div(j, NC), "c": lax.rem(j, NC)}

    def away(k):
        x = lax.rem(mxx + k // 2, NX)
        c = lax.rem(mc + k % 2, NC)
        return x * NC + c, {"x": x, "c": c}

    def back_to(k):
        return {"x": lax.rem(mxx + NX - k // 2, NX), "c": lax.rem(mc + k % 2, NC)}

    def tdev(d):
        return {"tp": tpeer(d)}

    def remote(src, dst, ssem, rsem, dev):
        return pltpu.make_async_remote_copy(
            src_ref=src,
            dst_ref=dst,
            send_sem=ssem,
            recv_sem=rsem,
            device_id=dev,
            device_id_type=MESH_IDS,
        )

    started = []

    def exchange(order, make):
        copies = [make(d) for d in order]
        for copy in copies:
            copy.start()
        started.extend(copies)
        return copies

    def arrived(copies):
        for copy in reversed(copies):
            copy.wait_recv()

    barrier = pltpu.get_barrier_semaphore()
    for d in Z_ORDER:
        pl.semaphore_signal(barrier, inc=1, device_id=zdev(d), device_id_type=MESH_IDS)
    for d in J_ORDER:
        pl.semaphore_signal(barrier, inc=1, device_id=jdev(d), device_id_type=MESH_IDS)
    for d in T_ORDER:
        pl.semaphore_signal(barrier, inc=1, device_id=tdev(d), device_id_type=MESH_IDS)

    inputs = [
        pltpu.make_async_copy(src, dst, in_sem.at[k])
        for k, (src, dst) in enumerate(
            (
                (tokens_in, tokens),
                (attn_gain_in, attn_gain),
                (wq_hbm, wq_in),
                (wk_hbm, wk_in),
                (wv_hbm, wv_in),
                (route_ids_in, route_ids),
                (route_weights_in, route_weights),
                (wo_hbm, wo_in),
                (ffn_gain_in, ffn_gain),
                (branch_gate_in, branch_gate),
                (bias_hbm, bias),
                (lengths_hbm, lengths),
            )
        )
    ]
    for copy in inputs:
        copy.start()
    kv_copies = []
    for s in range(0, 16, 2):
        kv_copies.append(
            pltpu.make_async_copy(
                keys_hbm.at[pl.ds(s, 2), 0], keys.at[pl.ds(s, 2)], kv_sem.at[s]
            )
        )
    for s in range(0, 16, 2):
        kv_copies.append(
            pltpu.make_async_copy(
                values_hbm.at[pl.ds(s, 2), 0], values.at[pl.ds(s, 2)], kv_sem.at[s + 1]
            )
        )
    for copy in kv_copies:
        copy.start()
    dense_col = pl.ds(pl.multiple_of(mj * 128, 128), 128)
    locals_ = [
        pltpu.make_async_copy(dgate_hbm, dgate.at[:, dense_col], local_sem.at[0]),
        pltpu.make_async_copy(dup_hbm, dup.at[:, dense_col], local_sem.at[1]),
        pltpu.make_async_copy(ddown_hbm, ddown.at[dense_col], local_sem.at[2]),
        pltpu.make_async_copy(egate_hbm.at[0], egate, local_sem.at[3]),
        pltpu.make_async_copy(eup_hbm.at[0], eup, local_sem.at[4]),
        pltpu.make_async_copy(edown_hbm.at[0], edown, local_sem.at[5]),
    ]
    for copy in locals_:
        copy.start()

    for copy in inputs[0:2]:
        copy.wait()
    tok = tokens[...].astype(F32)
    normed = (
        tok * lax.rsqrt(jnp.mean(tok * tok, axis=-1, keepdims=True) + norm_eps) * attn_gain[...]
    ).astype(BF)
    for z in range(NZ):
        nsend[z] = normed[:, 256 * z : 256 * (z + 1)]
    for copy in inputs[2:]:
        copy.wait()

    pl.semaphore_wait(barrier, NJ + NZ + NT - 3)

    def chunk_of(src, dst, k, lo, hi):
        return exchange(
            J_ORDER,
            lambda d: remote(
                src.at[:, lo:hi],
                dst.at[mj, :, lo:hi],
                j_send.at[k, d],
                j_recv.at[k, d],
                jdev(d),
            ),
        )

    c_wa = chunk_of(wq_in, wq, 0, 0, 256)
    c_n = exchange(
        Z_ORDER,
        lambda d: remote(
            nsend.at[zpeer(d)], nslab.at[mz], z_send.at[0, d], z_recv.at[0, d], zdev(d)
        ),
    )
    own_cols = pl.ds(pl.multiple_of(mt * 512, 512), 512)
    c_tok = exchange(
        Z_ORDER,
        lambda d: remote(
            tokens.at[:, own_cols],
            tok_all.at[mz, :, own_cols],
            z_send.at[4, d],
            z_recv.at[4, d],
            zdev(d),
        ),
    )
    c_wb = chunk_of(wq_in, wq, 1, 256, 512)
    c_wk = chunk_of(wk_in, wk, 2, 0, 128)
    c_wv = chunk_of(wv_in, wv, 9, 0, 128)
    c_wo = exchange(
        J_ORDER, lambda d: remote(wo_in, wo.at[mj], j_send.at[3, d], j_recv.at[3, d], jdev(d))
    )
    dense = (
        (dgate_hbm, lambda j: dgate.at[:, pl.ds(pl.multiple_of(j * 128, 128), 128)]),
        (dup_hbm, lambda j: dup.at[:, pl.ds(pl.multiple_of(j * 128, 128), 128)]),
        (ddown_hbm, lambda j: ddown.at[pl.ds(pl.multiple_of(j * 128, 128), 128)]),
    )
    c_dx = [
        exchange(
            (4, 2, 6),
            lambda d: remote(src, part(mj), j_send.at[4 + k, d], j_recv.at[4 + k, d], jdev(d)),
        )
        for k, (src, part) in enumerate(dense)
    ]
    partner = {"c": 1 - mc}
    c_dp = [
        exchange(
            (0,),
            lambda d: remote(src, part(mj), p_send.at[k, d], p_recv.at[k, d], partner),
        )
        for k, (src, part) in enumerate(dense)
    ]
    wq[mj] = wq_in[...]
    wk[mj] = wk_in[...]
    wv[mj] = wv_in[...]
    wo[mj] = wo_in[...]
    nslab[mz] = nsend[mz]
    tok_all[mz] = tokens[...]

    row_expert = lax.shift_right_logical(iota((128, 16), 0), 1)
    named = jnp.zeros((128, 16), F32)
    weighed = jnp.zeros((128, 16), F32)
    for k in range(4):
        hit = route_ids[k : k + 1, :] == row_expert
        named = named + one_if(hit)
        weighed = weighed + jnp.where(hit, route_weights[k : k + 1, :], 0.0)
    earlier = one_if(iota((16, 16), 0) < iota((16, 16), 1)).astype(BF)
    rank = dot(named.astype(BF), earlier)
    row_rank = jnp.bitwise_and(iota((128, 16), 0), 1).astype(F32)
    slots = jnp.where(rank == row_rank, weighed, 0.0)
    wd_all[mz] = jnp.concatenate([slots, jnp.zeros((128, 112), F32)], axis=1).T[0:16]

    def q_chunk(k, weight, lo, hi, at):
        width = hi - lo
        cols = slice(at, at + width)
        qsend[:, :, cols] = (
            dot(nslab[...].reshape(128, 256), weight[:, :, lo:hi].reshape(256, width))
            .astype(BF)
            .reshape(NZ, 16, width)
        )

    def q_exchange(k, lo, hi):
        copies = exchange(
            Z_ORDER,
            lambda d: remote(
                qsend.at[zpeer(d), :, lo:hi],
                qrecv.at[mz, :, lo:hi],
                z_send.at[k, d],
                z_recv.at[k, d],
                zdev(d),
            ),
        )
        qrecv[mz, :, lo:hi] = qsend[mz, :, lo:hi]
        return copies

    def q_sum(lo, hi):
        total = qrecv[0, :, lo:hi].astype(F32)
        for z in range(1, NZ):
            total = total + qrecv[z, :, lo:hi].astype(F32)
        return total.astype(BF)

    arrived(c_n)
    arrived(c_wa)
    q_chunk(0, wq, 0, 256, 0)
    c_qa = q_exchange(1, 0, 256)
    arrived(c_wb)
    q_chunk(1, wq, 256, 512, 256)
    c_qb = q_exchange(2, 256, 512)
    arrived(c_wk)
    arrived(c_wv)
    q_chunk(2, wk, 0, 128, 512)
    q_chunk(2, wv, 0, 128, 640)
    c_qc = q_exchange(3, 512, 768)
    c_wd = exchange(
        Z_ORDER,
        lambda d: remote(
            wd_all.at[mz], wd_all.at[mz], z_send.at[5, d], z_recv.at[5, d], zdev(d)
        ),
    )
    c_ftok = []
    for copy, d in reversed(list(zip(c_tok, Z_ORDER))):
        copy.wait_recv()
        block = tok_all.at[zsource(d), :, own_cols]
        c_ftok += exchange(
            T_ORDER,
            lambda e: remote(block, block, ft_send.at[d, e], ft_recv.at[d, e], tdev(e)),
        )

    for copy in kv_copies:
        copy.wait()
    arrived(c_qa)
    total_a = q_sum(0, 256)
    arrived(c_qb)
    total_b = q_sum(256, 512)

    q_rows = jnp.zeros((64, 128), F32)
    for h in range(4):
        part = (total_a, total_b)[h // 2][:, 128 * (h % 2) : 128 * (h % 2 + 1)]
        spread = one_if(iota((64, 16), 0) == 4 * iota((64, 16), 1) + h).astype(BF)
        q_rows = q_rows + dot(spread, part)
    q64[...] = q_rows
    first = iota((8, 128), 0) < 4
    for p in range(8):
        q8 = q64[8 * p : 8 * p + 8]
        qa = jnp.where(first, q8, 0.0).astype(BF)
        qb = jnp.where(first, 0.0, q8).astype(BF)
        scores[8 * p : 8 * p + 8] = dot_nt(qa, keys[2 * p]) + dot_nt(qb, keys[2 * p + 1])

    row = iota((64, 1), 0)
    head = jnp.bitwise_and(row, 3)
    seq = lax.shift_right_logical(row, 2)
    bias_col = jnp.zeros((64, 1), F32)
    for h in range(4):
        bias_col = jnp.where(head == h, bias[h], bias_col)
    len_col = jnp.zeros((64, 1), jnp.int32)
    for s in range(16):
        len_col = jnp.where(seq == s, lengths[s], len_col)
    after = one_if(iota((128, 128), 0) > iota((128, 128), 1)).astype(BF)
    carry = jnp.zeros((64, 1), F32)
    for b in reversed(range(8)):
        cols = slice(128 * b, 128 * (b + 1))
        zz = scores[:, cols] * (128 ** (-0.5)) + bias_col
        inside = (iota((64, 128), 1) + 128 * b) < len_col
        soft = jnp.log1p(jnp.exp(-jnp.abs(zz)))
        keep = jnp.where(inside, jnp.minimum(-zz, 0.0) - soft, 0.0)
        take = jnp.minimum(zz, 0.0) - soft
        k1 = keep.astype(BF)
        r1 = keep - k1.astype(F32)
        k2 = r1.astype(BF)
        k3 = (r1 - k2.astype(F32)).astype(BF)
        between = dot(k1, after) + dot(k2, after) + dot(k3, after) + carry
        carry = between[:, 0:1] + keep[:, 0:1]
        scores[:, cols] = jnp.where(inside, jnp.exp(take + between), 0.0)

    for p in range(8):
        w8 = scores[8 * p : 8 * p + 8].astype(BF)
        att64[8 * p : 8 * p + 8] = jnp.where(
            first, dot(w8, values[2 * p]), dot(w8, values[2 * p + 1])
        )
    att_rows = att64[...].astype(BF)
    for h in range(4):
        pick = one_if(iota((16, 64), 1) == 4 * iota((16, 64), 0) + h).astype(BF)
        att_all[mz, :, 128 * h : 128 * (h + 1)] = dot(pick, att_rows).astype(BF)

    c_a = exchange(
        Z_ORDER,
        lambda d: remote(
            att_all.at[mz], att_all.at[mz], z_send.at[6, d], z_recv.at[6, d], zdev(d)
        ),
    )
    arrived(c_qc)
    out[:, 512:768] = q_sum(512, 768)
    arrived(c_wd)
    slot_of_row = 16 * mz + 2 * lax.shift_right_logical(iota((128, 128), 0), 4)
    slot_of_row = slot_of_row + jnp.bitwise_and(iota((128, 128), 0), 1)
    spread = one_if(slot_of_row == iota((128, 128), 1)).astype(BF)
    row_z = jnp.bitwise_and(lax.shift_right_logical(iota((128, 128), 0), 1), 7)
    own_z = row_z == lax.shift_right_logical(iota((128, 128), 1), 4)
    wd = wd_all[...].reshape(128, 128)
    wd_hi = wd.astype(BF)
    wd_lo = (wd - wd_hi.astype(F32)).astype(BF)
    filled = one_if(wd > 0.0).astype(BF)
    dispatch = jnp.where(own_z, dot_nt(spread, filled), 0.0).astype(BF)
    row_z_t = jnp.bitwise_and(lax.shift_right_logical(iota((128, 128), 1), 1), 7)
    own_z_t = row_z_t == lax.shift_right_logical(iota((128, 128), 0), 4)
    comb_hi = jnp.where(own_z_t, dot_nt(wd_hi, spread), 0.0).astype(BF)
    comb_lo = jnp.where(own_z_t, dot_nt(wd_lo, spread), 0.0).astype(BF)
    arrived(c_wo)
    arrived(c_a)
    po_send[...] = (
        dot_nt(att_all[...].reshape(128, 512), wo[...].reshape(256, 512))
        .astype(BF)
        .reshape(NT, 32, 256)
    )
    c_po = exchange(
        T_ORDER,
        lambda d: remote(
            po_send.at[tpeer(d)], po_recv.at[mt], t_send.at[0, d], t_recv.at[0, d], tdev(d)
        ),
    )
    po_recv[mt] = po_send[mt]
    arrived(c_po)
    part = po_recv[0].astype(F32)
    for t in range(1, NT):
        part = part + po_recv[t].astype(F32)
    mixed[mt, mz] = part.astype(BF)

    own_block = mixed.at[mt, mz]
    c_mx = exchange(
        Z_ORDER,
        lambda d: remote(own_block, own_block, z_send.at[7, d], z_recv.at[7, d], zdev(d)),
    )
    c_fm = exchange(
        T_ORDER,
        lambda e: remote(own_block, own_block, fm_send.at[0, e], fm_recv.at[0, e], tdev(e)),
    )
    for k, (src, part) in enumerate(dense):
        arrived(c_dx[k])
        c_dp[k] += exchange(
            (2, 4, 6),
            lambda d: remote(
                part(lax.rem(mj + NJ - d, NJ)),
                part(lax.rem(mj + NJ - d, NJ)),
                p_send.at[k, d // 2],
                p_recv.at[k, d // 2],
                partner,
            ),
        )
    for copy, d in reversed(list(zip(c_mx, Z_ORDER))):
        copy.wait_recv()
        block = mixed.at[mt, zsource(d)]
        c_fm += exchange(
            T_ORDER,
            lambda e: remote(block, block, fm_send.at[d, e], fm_recv.at[d, e], tdev(e)),
        )
    for copy in c_ftok:
        copy.wait_recv()
    for copy in c_fm:
        copy.wait_recv()
    for z in range(NZ):
        pieces = []
        square = jnp.zeros((16, 1), F32)
        for s in range(NZ):
            cols = slice(256 * s, 256 * (s + 1))
            piece = tok_all[z, :, cols].astype(F32) + mixed[
                z // 2, s, 16 * (z % 2) : 16 * (z % 2) + 16
            ].astype(F32)
            square = square + jnp.sum(piece * piece, axis=-1, keepdims=True)
            pieces.append(piece)
        scale = lax.rsqrt(square * (1.0 / 2048) + norm_eps)
        for s in range(NZ):
            cols = slice(256 * s, 256 * (s + 1))
            xs[z, :, cols] = (pieces[s] * scale * ffn_gain[:, cols]).astype(BF)

    for b in range(4):
        cols = slice(512 * b, 512 * (b + 1))
        row_send[:, :, cols] = (
            dot(dispatch, xs[:, :, cols].reshape(128, 512)).astype(BF).reshape(NJ, 16, 512)
        )
    c_row = []
    for half, order in enumerate(((2, 6, 1), (4, 5, 3, 7))):
        c_row.append(
            exchange(
                order,
                lambda k: remote(
                    row_send.at[away(k)[0]],
                    row_recv.at[4 * half + HALVES[half].index(k)],
                    j_send.at[7, k],
                    j_recv.at[7, k],
                    away(k)[1],
                ),
            )
        )
    row_recv[0] = row_send[mj]

    for copy in locals_:
        copy.wait()
    arrived(c_dp[0])
    arrived(c_dp[1])
    x_own = xs[:, :, own_cols].reshape(128, 512)
    for t in range(NT):
        cols = slice(256 * t, 256 * (t + 1))
        pd_send[t, :, 0:256] = dot(x_own, dgate[:, cols]).astype(BF)
        pd_send[t, :, 256:512] = dot(x_own, dup[:, cols]).astype(BF)
    c_pd = exchange(
        T_ORDER,
        lambda d: remote(
            pd_send.at[tpeer(d)], pd_recv.at[mt], t_send.at[1, d], t_recv.at[1, d], tdev(d)
        ),
    )
    pd_recv[mt] = pd_send[mt]
    weighted = jnp.zeros((128, 128), F32)
    for r in range(16):
        weighted = weighted + (
            xs[:, :, 128 * r : 128 * (r + 1)].reshape(128, 128).astype(F32)
            * branch_gate[r : r + 1, :].astype(F32)
        )
    branch = jax.nn.sigmoid(jnp.sum(weighted, axis=-1, keepdims=True))
    c_pe = []
    for half in range(2):
        arrived(c_row[half])
        rows = row_recv[4 * half : 4 * half + 4].reshape(64, 2048)
        gate_c = jnp.minimum(dot(rows, egate[...]), clamp_limit)
        up_c = jnp.clip(dot(rows, eup[...]), -clamp_limit, clamp_limit)
        unit = ((up_c + 1.0) * gate_c * jax.nn.sigmoid(swish_alpha * gate_c)).astype(BF)
        for t in range(NT):
            pe_send[half, t] = dot(unit, edown[:, 512 * t : 512 * (t + 1)]).astype(BF)
        c_pe.append(
            exchange(
                T_ORDER,
                lambda d: remote(
                    pe_send.at[half, tpeer(d)],
                    pe_recv.at[half, mt],
                    t_send.at[3 + half, d],
                    t_recv.at[3 + half, d],
                    tdev(d),
                ),
            )
        )
        pe_recv[half, mt] = pe_send[half, mt]

    arrived(c_pd)
    pre = pd_recv[0].astype(F32)
    for t in range(1, NT):
        pre = pre + pd_recv[t].astype(F32)
    gate_d = pre[:, 0:256]
    hid[mt] = (gate_d * jax.nn.sigmoid(gate_d) * pre[:, 256:512]).astype(BF)
    c_h = exchange(
        T_ORDER,
        lambda d: remote(hid.at[mt], hid.at[mt], t_send.at[2, d], t_recv.at[2, d], tdev(d)),
    )

    c_er = []
    for half in range(2):
        arrived(c_pe[half])
        total_e = pe_recv[half, 0].astype(F32)
        for t in range(1, NT):
            total_e = total_e + pe_recv[half, t].astype(F32)
        er[4 * half : 4 * half + 4] = total_e.astype(BF).reshape(4, 16, 512)
        c_er += exchange(
            ((2, 6, 1), (4, 5, 3, 7))[half],
            lambda k: remote(
                er.at[4 * half + HALVES[half].index(k)],
                er_recv.at[mj],
                j_send.at[8, k],
                j_recv.at[8, k],
                back_to(k),
            ),
        )
    er_recv[mj] = er[0]

    arrived(c_h)
    arrived(c_dp[2])
    down = dot(hid[0], ddown[0:256])
    for t in range(1, NT):
        down = down + dot(hid[t], ddown[256 * t : 256 * (t + 1)])
    dense_part[...] = down * branch

    arrived(c_er)
    back = er_recv[...].reshape(128, 512)
    fin_send[...] = (
        (dot(comb_hi, back) + dot(comb_lo, back) + dense_part[...]).astype(BF).reshape(NZ, 16, 512)
    )
    c_f = exchange(
        Z_ORDER,
        lambda d: remote(
            fin_send.at[zpeer(d)], fin_recv.at[mz], z_send.at[8, d], z_recv.at[8, d], zdev(d)
        ),
    )
    fin_recv[mz] = fin_send[mz]
    quarter = lax.div(mz, 2)
    own_rows = pl.ds(pl.multiple_of(lax.rem(mz, 2) * 16, 16), 16)
    final = tokens[:, own_cols].astype(F32) + jnp.concatenate(
        [mixed[quarter, 2 * mt, own_rows], mixed[quarter, 2 * mt + 1, own_rows]], axis=1
    ).astype(F32)
    arrived(c_f)
    for z in range(NZ):
        final = final + fin_recv[z].astype(F32)
    out[:, 0:512] = final.astype(BF)

    for copy in started:
        copy.wait_send()


def split_kernel(both, layer_out, new_keys, new_values):
    layer_out[...] = both[:, 0:512]
    new_keys[...] = both[:, 512:640]
    new_values[...] = both[:, 640:768]


def body(
    tokens,
    attn_gain,
    query_weight,
    key_weight,
    value_weight,
    break_bias,
    cache_keys,
    cache_values,
    lengths,
    out_weight,
    ffn_gain,
    branch_gate,
    dense_gate,
    dense_up,
    dense_down,
    route_ids,
    route_weights,
    expert_gate,
    expert_up,
    expert_down,
):
    vm = pl.BlockSpec(memory_space=pltpu.VMEM)
    hbm = pl.BlockSpec(memory_space=pl.ANY)
    V = pltpu.VMEM
    D = pltpu.SemaphoreType.DMA
    both = pl.pallas_call(
        kernel,
        name="layer",
        out_shape=jax.ShapeDtypeStruct((16, 768), BF),
        in_specs=[hbm] * 20,
        out_specs=vm,
        scratch_shapes=[
            V((16, 2048), BF),
            V((1, 2048), F32),
            V((32, 512), BF),
            V((32, 128), BF),
            V((32, 128), BF),
            V((32, 512), BF),
            V((1, 2048), F32),
            V((16, 128), BF),
            V((4, 16), jnp.int32),
            V((4, 16), F32),
            pltpu.SMEM((4,), F32),
            pltpu.SMEM((16,), jnp.int32),
            V((16, 1024, 128), BF),
            V((16, 1024, 128), BF),
            V((2048, 256), BF),
            V((2048, 256), BF),
            V((256, 2048), BF),
            V((512, 1024), BF),
            V((512, 1024), BF),
            V((1024, 512), BF),
            V((NJ, 32, 512), BF),
            V((NJ, 32, 128), BF),
            V((NJ, 32, 128), BF),
            V((NJ, 32, 512), BF),
            V((NZ, 16, 256), BF),
            V((NZ, 16, 256), BF),
            V((NZ, 16, 768), BF),
            V((NZ, 16, 768), BF),
            V((64, 1024), F32),
            V((64, 128), F32),
            V((64, 128), F32),
            V((NZ, 16, 512), BF),
            V((NZ, 16, 128), F32),
            V((NZ, 16, 2048), BF),
            V((NT, 32, 256), BF),
            V((NT, 32, 256), BF),
            V((NT, NZ, 32, 256), BF),
            V((NZ, 16, 2048), BF),
            V((NJ, 16, 2048), BF),
            V((NJ, 16, 2048), BF),
            V((NT, 128, 512), BF),
            V((NT, 128, 512), BF),
            V((NT, 128, 256), BF),
            V((2, NT, 64, 512), BF),
            V((2, NT, 64, 512), BF),
            V((NJ, 16, 512), BF),
            V((NJ, 16, 512), BF),
            V((128, 512), F32),
            V((NZ, 16, 512), BF),
            V((NZ, 16, 512), BF),
            D((12,)),
            D((6,)),
            D((16,)),
            D((9, NZ)),
            D((9, NZ)),
            D((10, NJ)),
            D((10, NJ)),
            D((5, NT)),
            D((5, NT)),
            D((NZ, NT)),
            D((NZ, NT)),
            D((NZ, NT)),
            D((NZ, NT)),
            D((3, 4)),
            D((3, 4)),
        ],
        compiler_params=pltpu.CompilerParams(
            collective_id=0,
            has_side_effects=True,
            vmem_limit_bytes=60 * 1024 * 1024,
        ),
    )(
        tokens,
        attn_gain.reshape(1, -1),
        query_weight,
        key_weight,
        value_weight,
        break_bias,
        cache_keys,
        cache_values,
        lengths,
        out_weight.T,
        ffn_gain.reshape(1, -1),
        branch_gate.reshape(16, 128),
        dense_gate,
        dense_up,
        dense_down,
        route_ids.T,
        route_weights.T,
        expert_gate,
        expert_up,
        expert_down,
    )
    return tuple(
        pl.pallas_call(
            split_kernel,
            name="split",
            out_shape=(
                jax.ShapeDtypeStruct((16, 512), BF),
                jax.ShapeDtypeStruct((16, 128), BF),
                jax.ShapeDtypeStruct((16, 128), BF),
            ),
            in_specs=[vm],
            out_specs=(vm, vm, vm),
        )(both)
    )


def solution(mesh):
    split = Mesh(mesh.devices.reshape(NZ, NX, NC, NT), ("z", "x", "c", "tp"))
    return jax.shard_map(
        body,
        mesh=split,
        in_specs=(
            P(EP, None),
            P(),
            P(EP, "tp"),
            P(EP, "tp"),
            P(EP, "tp"),
            P("tp"),
            P(EP, "tp", None, None),
            P(EP, "tp", None, None),
            P(EP),
            P("tp", EP),
            P(),
            P(),
            P("tp", EP),
            P("tp", EP),
            P(EP, "tp"),
            P(EP, None),
            P(EP, None),
            P(EP, None, "tp"),
            P(EP, None, "tp"),
            P(EP, "tp", None),
        ),
        out_specs=(P(EP, "tp"), P(EP, "tp"), P(EP, "tp")),
        check_vma=False,
    )
```

```python
import functools

import jax
import jax.numpy as jnp
from jax import lax
from jax.experimental import pallas as pl
from jax.experimental.pallas import tpu as pltpu
from jax.sharding import Mesh
from jax.sharding import PartitionSpec as P

EP = ("z", "x", "c")
NZ, NX, NC, NT = 8, 4, 2, 4
NJ = NX * NC

norm_eps = 1e-05
clamp_limit = 7.0
swish_alpha = 1.702

BF = jnp.bfloat16
F32 = jnp.float32
MESH_IDS = pl.DeviceIdType.MESH


def dot(a, b):
    return jnp.dot(a, b, preferred_element_type=F32)


def dot_nt(a, b):
    return lax.dot_general(a, b, (((1,), (1,)), ((), ())), preferred_element_type=F32)


def iota(shape, dim):
    return lax.broadcasted_iota(jnp.int32, shape, dim)


def one_if(mask):
    return jnp.where(mask, 1.0, 0.0)


Z_ORDER = (4, 3, 5, 2, 6, 1, 7)
J_ORDER = (4, 3, 5, 2, 6, 1, 7)
T_ORDER = (2, 1, 3)
HALVES = ((0, 1, 2, 6), (4, 5, 3, 7))


def kernel(
    tokens_in,
    attn_gain_in,
    wq_hbm,
    wk_hbm,
    wv_hbm,
    bias_hbm,
    keys_hbm,
    values_hbm,
    lengths_hbm,
    wo_hbm,
    ffn_gain_in,
    branch_gate_in,
    dgate_hbm,
    dup_hbm,
    ddown_hbm,
    route_ids_in,
    route_weights_in,
    egate_hbm,
    eup_hbm,
    edown_hbm,
    out,
    tokens,
    attn_gain,
    wq_in,
    wk_in,
    wv_in,
    wo_in,
    ffn_gain,
    branch_gate,
    route_ids,
    route_weights,
    bias,
    lengths,
    keys,
    values,
    egate,
    eup,
    edown,
    dgate,
    dup,
    ddown,
    wq,
    wk,
    wv,
    wo,
    nsend,
    nslab,
    qsend,
    qrecv,
    scores,
    q64,
    att64,
    att_all,
    wd_all,
    tok_all,
    po_send,
    po_recv,
    mixed,
    xs,
    row_send,
    row_recv,
    pd_send,
    pd_recv,
    hid,
    pe_send,
    pe_recv,
    er,
    er_recv,
    dense_part,
    fin_send,
    fin_recv,
    in_sem,
    local_sem,
    kv_sem,
    z_send,
    z_recv,
    j_send,
    j_recv,
    t_send,
    t_recv,
    ft_send,
    ft_recv,
    fm_send,
    fm_recv,
    p_send,
    p_recv,
):
    mz = lax.axis_index("z")
    mxx = lax.axis_index("x")
    mc = lax.axis_index("c")
    mt = lax.axis_index("tp")
    mj = mxx * NC + mc

    def zpeer(d):
        return lax.rem(mz + d, NZ)

    def zsource(d):
        return lax.rem(mz + NZ - d, NZ)

    def jpeer(d):
        return lax.rem(mj + d, NJ)

    def tpeer(d):
        return lax.rem(mt + d, NT)

    def zdev(d):
        return {"z": zpeer(d)}

    def jdev(d):
        j = jpeer(d)
        return {"x": lax.div(j, NC), "c": lax.rem(j, NC)}

    def away(k):
        x = lax.rem(mxx + k // 2, NX)
        c = lax.rem(mc + k % 2, NC)
        return x * NC + c, {"x": x, "c": c}

    def back_to(k):
        return {"x": lax.rem(mxx + NX - k // 2, NX), "c": lax.rem(mc + k % 2, NC)}

    def tdev(d):
        return {"tp": tpeer(d)}

    def remote(src, dst, ssem, rsem, dev):
        return pltpu.make_async_remote_copy(
            src_ref=src,
            dst_ref=dst,
            send_sem=ssem,
            recv_sem=rsem,
            device_id=dev,
            device_id_type=MESH_IDS,
        )

    started = []

    def exchange(order, make):
        copies = [make(d) for d in order]
        for copy in copies:
            copy.start()
        started.extend(copies)
        return copies

    def arrived(copies):
        for copy in reversed(copies):
            copy.wait_recv()

    barrier = pltpu.get_barrier_semaphore()
    for d in Z_ORDER:
        pl.semaphore_signal(barrier, inc=1, device_id=zdev(d), device_id_type=MESH_IDS)
    for d in J_ORDER:
        pl.semaphore_signal(barrier, inc=1, device_id=jdev(d), device_id_type=MESH_IDS)
    for d in T_ORDER:
        pl.semaphore_signal(barrier, inc=1, device_id=tdev(d), device_id_type=MESH_IDS)

    inputs = [
        pltpu.make_async_copy(src, dst, in_sem.at[k])
        for k, (src, dst) in enumerate(
            (
                (tokens_in, tokens),
                (attn_gain_in, attn_gain),
                (wq_hbm, wq_in),
                (wk_hbm, wk_in),
                (wv_hbm, wv_in),
                (route_ids_in, route_ids),
                (route_weights_in, route_weights),
                (wo_hbm, wo_in),
                (ffn_gain_in, ffn_gain),
                (branch_gate_in, branch_gate),
                (bias_hbm, bias),
                (lengths_hbm, lengths),
            )
        )
    ]
    for copy in inputs:
        copy.start()
    kv_copies = []
    for s in range(0, 16, 2):
        kv_copies.append(
            pltpu.make_async_copy(
                keys_hbm.at[pl.ds(s, 2), 0], keys.at[pl.ds(s, 2)], kv_sem.at[s]
            )
        )
    for s in range(0, 16, 2):
        kv_copies.append(
            pltpu.make_async_copy(
                values_hbm.at[pl.ds(s, 2), 0], values.at[pl.ds(s, 2)], kv_sem.at[s + 1]
            )
        )
    for copy in kv_copies:
        copy.start()
    dense_col = pl.ds(pl.multiple_of(mj * 128, 128), 128)
    locals_ = [
        pltpu.make_async_copy(dgate_hbm, dgate.at[:, dense_col], local_sem.at[0]),
        pltpu.make_async_copy(dup_hbm, dup.at[:, dense_col], local_sem.at[1]),
        pltpu.make_async_copy(ddown_hbm, ddown.at[dense_col], local_sem.at[2]),
        pltpu.make_async_copy(egate_hbm.at[0], egate, local_sem.at[3]),
        pltpu.make_async_copy(eup_hbm.at[0], eup, local_sem.at[4]),
        pltpu.make_async_copy(edown_hbm.at[0], edown, local_sem.at[5]),
    ]
    for copy in locals_:
        copy.start()

    inputs[2].wait()

    pl.semaphore_wait(barrier, NJ + NZ + NT - 3)

    def chunk_of(src, dst, k, lo, hi):
        return exchange(
            J_ORDER,
            lambda d: remote(
                src.at[:, lo:hi],
                dst.at[mj, :, lo:hi],
                j_send.at[k, d],
                j_recv.at[k, d],
                jdev(d),
            ),
        )

    c_wa = chunk_of(wq_in, wq, 0, 0, 256)
    for copy in inputs[0:2]:
        copy.wait()
    tok = tokens[...].astype(F32)
    normed = (
        tok * lax.rsqrt(jnp.mean(tok * tok, axis=-1, keepdims=True) + norm_eps) * attn_gain[...]
    ).astype(BF)
    for z in range(NZ):
        nsend[z] = normed[:, 256 * z : 256 * (z + 1)]
    c_n = exchange(
        Z_ORDER,
        lambda d: remote(
            nsend.at[zpeer(d)], nslab.at[mz], z_send.at[0, d], z_recv.at[0, d], zdev(d)
        ),
    )
    own_cols = pl.ds(pl.multiple_of(mt * 512, 512), 512)
    c_tok = exchange(
        Z_ORDER,
        lambda d: remote(
            tokens.at[:, own_cols],
            tok_all.at[mz, :, own_cols],
            z_send.at[4, d],
            z_recv.at[4, d],
            zdev(d),
        ),
    )
    c_wb = chunk_of(wq_in, wq, 1, 256, 512)
    for copy in inputs[3:]:
        copy.wait()
    c_wk = chunk_of(wk_in, wk, 2, 0, 128)
    c_wv = chunk_of(wv_in, wv, 9, 0, 128)
    c_wo = exchange(
        J_ORDER, lambda d: remote(wo_in, wo.at[mj], j_send.at[3, d], j_recv.at[3, d], jdev(d))
    )
    dense = (
        (dgate_hbm, lambda j: dgate.at[:, pl.ds(pl.multiple_of(j * 128, 128), 128)]),
        (dup_hbm, lambda j: dup.at[:, pl.ds(pl.multiple_of(j * 128, 128), 128)]),
        (ddown_hbm, lambda j: ddown.at[pl.ds(pl.multiple_of(j * 128, 128), 128)]),
    )
    c_dx = [
        exchange(
            (4, 2, 6),
            lambda d: remote(src, part(mj), j_send.at[4 + k, d], j_recv.at[4 + k, d], jdev(d)),
        )
        for k, (src, part) in enumerate(dense)
    ]
    partner = {"c": 1 - mc}
    c_dp = [
        exchange(
            (0,),
            lambda d: remote(src, part(mj), p_send.at[k, d], p_recv.at[k, d], partner),
        )
        for k, (src, part) in enumerate(dense)
    ]
    wq[mj] = wq_in[...]
    wk[mj] = wk_in[...]
    wv[mj] = wv_in[...]
    wo[mj] = wo_in[...]
    nslab[mz] = nsend[mz]
    tok_all[mz] = tokens[...]

    row_expert = lax.shift_right_logical(iota((128, 16), 0), 1)
    named = jnp.zeros((128, 16), F32)
    weighed = jnp.zeros((128, 16), F32)
    for k in range(4):
        hit = route_ids[k : k + 1, :] == row_expert
        named = named + one_if(hit)
        weighed = weighed + jnp.where(hit, route_weights[k : k + 1, :], 0.0)
    earlier = one_if(iota((16, 16), 0) < iota((16, 16), 1)).astype(BF)
    rank = dot(named.astype(BF), earlier)
    row_rank = jnp.bitwise_and(iota((128, 16), 0), 1).astype(F32)
    slots = jnp.where(rank == row_rank, weighed, 0.0)
    wd_all[mz] = jnp.concatenate([slots, jnp.zeros((128, 112), F32)], axis=1).T[0:16]

    def q_chunk(k, weight, lo, hi, at):
        width = hi - lo
        cols = slice(at, at + width)
        qsend[:, :, cols] = (
            dot(nslab[...].reshape(128, 256), weight[:, :, lo:hi].reshape(256, width))
            .astype(BF)
            .reshape(NZ, 16, width)
        )

    def q_exchange(k, lo, hi):
        copies = exchange(
            Z_ORDER,
            lambda d: remote(
                qsend.at[zpeer(d), :, lo:hi],
                qrecv.at[mz, :, lo:hi],
                z_send.at[k, d],
                z_recv.at[k, d],
                zdev(d),
            ),
        )
        qrecv[mz, :, lo:hi] = qsend[mz, :, lo:hi]
        return copies

    def q_sum(lo, hi):
        total = qrecv[0, :, lo:hi].astype(F32)
        for z in range(1, NZ):
            total = total + qrecv[z, :, lo:hi].astype(F32)
        return total.astype(BF)

    arrived(c_n)
    arrived(c_wa)
    q_chunk(0, wq, 0, 256, 0)
    c_qa = q_exchange(1, 0, 256)
    arrived(c_wb)
    q_chunk(1, wq, 256, 512, 256)
    c_qb = q_exchange(2, 256, 512)
    arrived(c_wk)
    arrived(c_wv)
    q_chunk(2, wk, 0, 128, 512)
    q_chunk(2, wv, 0, 128, 640)
    c_qc = q_exchange(3, 512, 768)
    c_wd = exchange(
        Z_ORDER,
        lambda d: remote(
            wd_all.at[mz], wd_all.at[mz], z_send.at[5, d], z_recv.at[5, d], zdev(d)
        ),
    )
    c_ftok = []
    for copy, d in reversed(list(zip(c_tok, Z_ORDER))):
        copy.wait_recv()
        block = tok_all.at[zsource(d), :, own_cols]
        c_ftok += exchange(
            T_ORDER,
            lambda e: remote(block, block, ft_send.at[d, e], ft_recv.at[d, e], tdev(e)),
        )

    for copy in kv_copies:
        copy.wait()
    arrived(c_qa)
    total_a = q_sum(0, 256)
    arrived(c_qb)
    total_b = q_sum(256, 512)

    q_rows = jnp.zeros((64, 128), F32)
    for h in range(4):
        part = (total_a, total_b)[h // 2][:, 128 * (h % 2) : 128 * (h % 2 + 1)]
        spread = one_if(iota((64, 16), 0) == 4 * iota((64, 16), 1) + h).astype(BF)
        q_rows = q_rows + dot(spread, part)
    q64[...] = q_rows
    first = iota((8, 128), 0) < 4
    for p in range(8):
        q8 = q64[8 * p : 8 * p + 8]
        qa = jnp.where(first, q8, 0.0).astype(BF)
        qb = jnp.where(first, 0.0, q8).astype(BF)
        scores[8 * p : 8 * p + 8] = dot_nt(qa, keys[2 * p]) + dot_nt(qb, keys[2 * p + 1])

    row = iota((64, 1), 0)
    head = jnp.bitwise_and(row, 3)
    seq = lax.shift_right_logical(row, 2)
    bias_col = jnp.zeros((64, 1), F32)
    for h in range(4):
        bias_col = jnp.where(head == h, bias[h], bias_col)
    len_col = jnp.zeros((64, 1), jnp.int32)
    for s in range(16):
        len_col = jnp.where(seq == s, lengths[s], len_col)
    after = one_if(iota((128, 128), 0) > iota((128, 128), 1)).astype(BF)
    carry = jnp.zeros((64, 1), F32)
    for b in reversed(range(8)):
        cols = slice(128 * b, 128 * (b + 1))
        zz = scores[:, cols] * (128 ** (-0.5)) + bias_col
        inside = (iota((64, 128), 1) + 128 * b) < len_col
        soft = jnp.log1p(jnp.exp(-jnp.abs(zz)))
        keep = jnp.where(inside, jnp.minimum(-zz, 0.0) - soft, 0.0)
        take = jnp.minimum(zz, 0.0) - soft
        k1 = keep.astype(BF)
        r1 = keep - k1.astype(F32)
        k2 = r1.astype(BF)
        k3 = (r1 - k2.astype(F32)).astype(BF)
        between = dot(k1, after) + dot(k2, after) + dot(k3, after) + carry
        carry = between[:, 0:1] + keep[:, 0:1]
        scores[:, cols] = jnp.where(inside, jnp.exp(take + between), 0.0)

    for p in range(8):
        w8 = scores[8 * p : 8 * p + 8].astype(BF)
        att64[8 * p : 8 * p + 8] = jnp.where(
            first, dot(w8, values[2 * p]), dot(w8, values[2 * p + 1])
        )
    att_rows = att64[...].astype(BF)
    for h in range(4):
        pick = one_if(iota((16, 64), 1) == 4 * iota((16, 64), 0) + h).astype(BF)
        att_all[mz, :, 128 * h : 128 * (h + 1)] = dot(pick, att_rows).astype(BF)

    c_a = exchange(
        Z_ORDER,
        lambda d: remote(
            att_all.at[mz], att_all.at[mz], z_send.at[6, d], z_recv.at[6, d], zdev(d)
        ),
    )
    arrived(c_qc)
    out[:, 512:768] = q_sum(512, 768)
    arrived(c_wd)
    slot_of_row = 16 * mz + 2 * lax.shift_right_logical(iota((128, 128), 0), 4)
    slot_of_row = slot_of_row + jnp.bitwise_and(iota((128, 128), 0), 1)
    spread = one_if(slot_of_row == iota((128, 128), 1)).astype(BF)
    row_z = jnp.bitwise_and(lax.shift_right_logical(iota((128, 128), 0), 1), 7)
    own_z = row_z == lax.shift_right_logical(iota((128, 128), 1), 4)
    wd = wd_all[...].reshape(128, 128)
    wd_hi = wd.astype(BF)
    wd_lo = (wd - wd_hi.astype(F32)).astype(BF)
    filled = one_if(wd > 0.0).astype(BF)
    dispatch = jnp.where(own_z, dot_nt(spread, filled), 0.0).astype(BF)
    row_z_t = jnp.bitwise_and(lax.shift_right_logical(iota((128, 128), 1), 1), 7)
    own_z_t = row_z_t == lax.shift_right_logical(iota((128, 128), 0), 4)
    comb_hi = jnp.where(own_z_t, dot_nt(wd_hi, spread), 0.0).astype(BF)
    comb_lo = jnp.where(own_z_t, dot_nt(wd_lo, spread), 0.0).astype(BF)
    arrived(c_wo)
    arrived(c_a)
    po_send[...] = (
        dot_nt(att_all[...].reshape(128, 512), wo[...].reshape(256, 512))
        .astype(BF)
        .reshape(NT, 32, 256)
    )
    c_po = exchange(
        T_ORDER,
        lambda d: remote(
            po_send.at[tpeer(d)], po_recv.at[mt], t_send.at[0, d], t_recv.at[0, d], tdev(d)
        ),
    )
    po_recv[mt] = po_send[mt]
    arrived(c_po)
    part = po_recv[0].astype(F32)
    for t in range(1, NT):
        part = part + po_recv[t].astype(F32)
    mixed[mt, mz] = part.astype(BF)

    own_block = mixed.at[mt, mz]
    c_mx = exchange(
        Z_ORDER,
        lambda d: remote(own_block, own_block, z_send.at[7, d], z_recv.at[7, d], zdev(d)),
    )
    c_fm = exchange(
        T_ORDER,
        lambda e: remote(own_block, own_block, fm_send.at[0, e], fm_recv.at[0, e], tdev(e)),
    )
    for copy, d in reversed(list(zip(c_mx, Z_ORDER))):
        copy.wait_recv()
        block = mixed.at[mt, zsource(d)]
        c_fm += exchange(
            T_ORDER,
            lambda e: remote(block, block, fm_send.at[d, e], fm_recv.at[d, e], tdev(e)),
        )
    for k, (src, part) in enumerate(dense):
        arrived(c_dx[k])
        c_dp[k] += exchange(
            (2, 4, 6),
            lambda d: remote(
                part(lax.rem(mj + NJ - d, NJ)),
                part(lax.rem(mj + NJ - d, NJ)),
                p_send.at[k, d // 2],
                p_recv.at[k, d // 2],
                partner,
            ),
        )
    for copy in c_ftok:
        copy.wait_recv()
    for copy in c_fm:
        copy.wait_recv()
    for z in range(NZ):
        pieces = []
        square = jnp.zeros((16, 1), F32)
        for s in range(NZ):
            cols = slice(256 * s, 256 * (s + 1))
            piece = tok_all[z, :, cols].astype(F32) + mixed[
                z // 2, s, 16 * (z % 2) : 16 * (z % 2) + 16
            ].astype(F32)
            square = square + jnp.sum(piece * piece, axis=-1, keepdims=True)
            pieces.append(piece)
        scale = lax.rsqrt(square * (1.0 / 2048) + norm_eps)
        for s in range(NZ):
            cols = slice(256 * s, 256 * (s + 1))
            xs[z, :, cols] = (pieces[s] * scale * ffn_gain[:, cols]).astype(BF)

    for copy in locals_:
        copy.wait()
    arrived(c_dp[0])
    arrived(c_dp[1])
    x_own = xs[:, :, own_cols].reshape(128, 512)
    c_pd = []
    for d in T_ORDER + (0,):
        to = tpeer(d)
        cols = pl.ds(pl.multiple_of(to * 256, 256), 256)
        block = pd_recv if d == 0 else pd_send
        block[to, :, 0:256] = dot(x_own, dgate[:, cols]).astype(BF)
        block[to, :, 256:512] = dot(x_own, dup[:, cols]).astype(BF)
        if d > 0:
            c_pd += exchange(
                (d,),
                lambda d: remote(
                    pd_send.at[to], pd_recv.at[mt], t_send.at[1, d], t_recv.at[1, d], tdev(d)
                ),
            )

    for b in range(4):
        cols = slice(512 * b, 512 * (b + 1))
        row_send[:, :, cols] = (
            dot(dispatch, xs[:, :, cols].reshape(128, 512)).astype(BF).reshape(NJ, 16, 512)
        )
    c_row = []
    for half, order in enumerate(((2, 6, 1), (4, 5, 3, 7))):
        c_row.append(
            exchange(
                order,
                lambda k: remote(
                    row_send.at[away(k)[0]],
                    row_recv.at[4 * half + HALVES[half].index(k)],
                    j_send.at[7, k],
                    j_recv.at[7, k],
                    away(k)[1],
                ),
            )
        )
    row_recv[0] = row_send[mj]

    weighted = jnp.zeros((128, 128), F32)
    for r in range(16):
        weighted = weighted + (
            xs[:, :, 128 * r : 128 * (r + 1)].reshape(128, 128).astype(F32)
            * branch_gate[r : r + 1, :].astype(F32)
        )
    branch = jax.nn.sigmoid(jnp.sum(weighted, axis=-1, keepdims=True))
    c_pe = []
    for half in range(2):
        arrived(c_row[half])
        rows = row_recv[4 * half : 4 * half + 4].reshape(64, 2048)
        gate_c = jnp.minimum(dot(rows, egate[...]), clamp_limit)
        up_c = jnp.clip(dot(rows, eup[...]), -clamp_limit, clamp_limit)
        unit = ((up_c + 1.0) * gate_c * jax.nn.sigmoid(swish_alpha * gate_c)).astype(BF)
        for t in range(NT):
            pe_send[half, t] = dot(unit, edown[:, 512 * t : 512 * (t + 1)]).astype(BF)
        c_pe.append(
            exchange(
                T_ORDER,
                lambda d: remote(
                    pe_send.at[half, tpeer(d)],
                    pe_recv.at[half, mt],
                    t_send.at[3 + half, d],
                    t_recv.at[3 + half, d],
                    tdev(d),
                ),
            )
        )
        pe_recv[half, mt] = pe_send[half, mt]

    arrived(c_pd)
    pre = pd_recv[0].astype(F32)
    for t in range(1, NT):
        pre = pre + pd_recv[t].astype(F32)
    gate_d = pre[:, 0:256]
    hid[mt] = (gate_d * jax.nn.sigmoid(gate_d) * pre[:, 256:512]).astype(BF)
    c_h = exchange(
        T_ORDER,
        lambda d: remote(hid.at[mt], hid.at[mt], t_send.at[2, d], t_recv.at[2, d], tdev(d)),
    )

    c_er = []
    for half in range(2):
        arrived(c_pe[half])
        total_e = pe_recv[half, 0].astype(F32)
        for t in range(1, NT):
            total_e = total_e + pe_recv[half, t].astype(F32)
        er[4 * half : 4 * half + 4] = total_e.astype(BF).reshape(4, 16, 512)
        c_er += exchange(
            ((2, 6, 1), (4, 5, 3, 7))[half],
            lambda k: remote(
                er.at[4 * half + HALVES[half].index(k)],
                er_recv.at[mj],
                j_send.at[8, k],
                j_recv.at[8, k],
                back_to(k),
            ),
        )
    er_recv[mj] = er[0]

    arrived(c_h)
    arrived(c_dp[2])
    down = dot(hid[0], ddown[0:256])
    for t in range(1, NT):
        down = down + dot(hid[t], ddown[256 * t : 256 * (t + 1)])
    dense_part[...] = down * branch

    arrived(c_er)
    back = er_recv[...].reshape(128, 512)
    fin_send[...] = (
        (dot(comb_hi, back) + dot(comb_lo, back) + dense_part[...]).astype(BF).reshape(NZ, 16, 512)
    )
    c_f = exchange(
        Z_ORDER,
        lambda d: remote(
            fin_send.at[zpeer(d)], fin_recv.at[mz], z_send.at[8, d], z_recv.at[8, d], zdev(d)
        ),
    )
    fin_recv[mz] = fin_send[mz]
    quarter = lax.div(mz, 2)
    own_rows = pl.ds(pl.multiple_of(lax.rem(mz, 2) * 16, 16), 16)
    final = tokens[:, own_cols].astype(F32) + jnp.concatenate(
        [mixed[quarter, 2 * mt, own_rows], mixed[quarter, 2 * mt + 1, own_rows]], axis=1
    ).astype(F32)
    for copy in started[: -len(c_f)]:
        copy.wait_send()
    arrived(c_f)
    for z in range(NZ):
        final = final + fin_recv[z].astype(F32)
    out[:, 0:512] = final.astype(BF)

    for copy in c_f:
        copy.wait_send()


def split_kernel(both, layer_out, new_keys, new_values):
    layer_out[...] = both[:, 0:512]
    new_keys[...] = both[:, 512:640]
    new_values[...] = both[:, 640:768]


def body(
    tokens,
    attn_gain,
    query_weight,
    key_weight,
    value_weight,
    break_bias,
    cache_keys,
    cache_values,
    lengths,
    out_weight,
    ffn_gain,
    branch_gate,
    dense_gate,
    dense_up,
    dense_down,
    route_ids,
    route_weights,
    expert_gate,
    expert_up,
    expert_down,
):
    vm = pl.BlockSpec(memory_space=pltpu.VMEM)
    hbm = pl.BlockSpec(memory_space=pl.ANY)
    V = pltpu.VMEM
    D = pltpu.SemaphoreType.DMA
    both = pl.pallas_call(
        kernel,
        name="layer",
        out_shape=jax.ShapeDtypeStruct((16, 768), BF),
        in_specs=[hbm] * 20,
        out_specs=vm,
        scratch_shapes=[
            V((16, 2048), BF),
            V((1, 2048), F32),
            V((32, 512), BF),
            V((32, 128), BF),
            V((32, 128), BF),
            V((32, 512), BF),
            V((1, 2048), F32),
            V((16, 128), BF),
            V((4, 16), jnp.int32),
            V((4, 16), F32),
            pltpu.SMEM((4,), F32),
            pltpu.SMEM((16,), jnp.int32),
            V((16, 1024, 128), BF),
            V((16, 1024, 128), BF),
            V((2048, 256), BF),
            V((2048, 256), BF),
            V((256, 2048), BF),
            V((512, 1024), BF),
            V((512, 1024), BF),
            V((1024, 512), BF),
            V((NJ, 32, 512), BF),
            V((NJ, 32, 128), BF),
            V((NJ, 32, 128), BF),
            V((NJ, 32, 512), BF),
            V((NZ, 16, 256), BF),
            V((NZ, 16, 256), BF),
            V((NZ, 16, 768), BF),
            V((NZ, 16, 768), BF),
            V((64, 1024), F32),
            V((64, 128), F32),
            V((64, 128), F32),
            V((NZ, 16, 512), BF),
            V((NZ, 16, 128), F32),
            V((NZ, 16, 2048), BF),
            V((NT, 32, 256), BF),
            V((NT, 32, 256), BF),
            V((NT, NZ, 32, 256), BF),
            V((NZ, 16, 2048), BF),
            V((NJ, 16, 2048), BF),
            V((NJ, 16, 2048), BF),
            V((NT, 128, 512), BF),
            V((NT, 128, 512), BF),
            V((NT, 128, 256), BF),
            V((2, NT, 64, 512), BF),
            V((2, NT, 64, 512), BF),
            V((NJ, 16, 512), BF),
            V((NJ, 16, 512), BF),
            V((128, 512), F32),
            V((NZ, 16, 512), BF),
            V((NZ, 16, 512), BF),
            D((12,)),
            D((6,)),
            D((16,)),
            D((9, NZ)),
            D((9, NZ)),
            D((10, NJ)),
            D((10, NJ)),
            D((5, NT)),
            D((5, NT)),
            D((NZ, NT)),
            D((NZ, NT)),
            D((NZ, NT)),
            D((NZ, NT)),
            D((3, 4)),
            D((3, 4)),
        ],
        compiler_params=pltpu.CompilerParams(
            collective_id=0,
            has_side_effects=True,
            vmem_limit_bytes=60 * 1024 * 1024,
        ),
    )(
        tokens,
        attn_gain.reshape(1, -1),
        query_weight,
        key_weight,
        value_weight,
        break_bias,
        cache_keys,
        cache_values,
        lengths,
        out_weight.T,
        ffn_gain.reshape(1, -1),
        branch_gate.reshape(16, 128),
        dense_gate,
        dense_up,
        dense_down,
        route_ids.T,
        route_weights.T,
        expert_gate,
        expert_up,
        expert_down,
    )
    return tuple(
        pl.pallas_call(
            split_kernel,
            name="split",
            out_shape=(
                jax.ShapeDtypeStruct((16, 512), BF),
                jax.ShapeDtypeStruct((16, 128), BF),
                jax.ShapeDtypeStruct((16, 128), BF),
            ),
            in_specs=[vm],
            out_specs=(vm, vm, vm),
        )(both)
    )


def solution(mesh):
    split = Mesh(mesh.devices.reshape(NZ, NX, NC, NT), ("z", "x", "c", "tp"))
    return jax.shard_map(
        body,
        mesh=split,
        in_specs=(
            P(EP, None),
            P(),
            P(EP, "tp"),
            P(EP, "tp"),
            P(EP, "tp"),
            P("tp"),
            P(EP, "tp", None, None),
            P(EP, "tp", None, None),
            P(EP),
            P("tp", EP),
            P(),
            P(),
            P("tp", EP),
            P("tp", EP),
            P(EP, "tp"),
            P(EP, None),
            P(EP, None),
            P(EP, None, "tp"),
            P(EP, None, "tp"),
            P(EP, "tp", None),
        ),
        out_specs=(P(EP, "tp"), P(EP, "tp"), P(EP, "tp")),
        check_vma=False,
    )
```

```python
import functools

import jax
import jax.numpy as jnp
from jax import lax
from jax.experimental import pallas as pl
from jax.experimental.pallas import tpu as pltpu
from jax.sharding import Mesh
from jax.sharding import PartitionSpec as P

EP = ("z", "x", "c")
NZ, NX, NC, NT = 8, 4, 2, 4
NJ = NX * NC

norm_eps = 1e-05
clamp_limit = 7.0
swish_alpha = 1.702

BF = jnp.bfloat16
F32 = jnp.float32
MESH_IDS = pl.DeviceIdType.MESH


def dot(a, b):
    return jnp.dot(a, b, preferred_element_type=F32)


def dot_nt(a, b):
    return lax.dot_general(a, b, (((1,), (1,)), ((), ())), preferred_element_type=F32)


def iota(shape, dim):
    return lax.broadcasted_iota(jnp.int32, shape, dim)


def one_if(mask):
    return jnp.where(mask, 1.0, 0.0)


Z_ORDER = (4, 3, 5, 2, 6, 1, 7)
J_ORDER = (4, 3, 5, 2, 6, 1, 7)
T_ORDER = (2, 1, 3)
HALVES = ((0, 1, 2, 6), (4, 5, 3, 7))


def kernel(
    tokens_in,
    attn_gain_in,
    wq_hbm,
    wk_hbm,
    wv_hbm,
    bias_hbm,
    keys_hbm,
    values_hbm,
    lengths_hbm,
    wo_hbm,
    ffn_gain_in,
    branch_gate_in,
    dgate_hbm,
    dup_hbm,
    ddown_hbm,
    route_ids_in,
    route_weights_in,
    egate_hbm,
    eup_hbm,
    edown_hbm,
    out,
    tokens,
    attn_gain,
    wq_in,
    wk_in,
    wv_in,
    wo_in,
    ffn_gain,
    branch_gate,
    route_ids,
    route_weights,
    bias,
    lengths,
    keys,
    values,
    egate,
    eup,
    edown,
    dgate,
    dup,
    ddown,
    wq,
    wk,
    wv,
    wo,
    nsend,
    nslab,
    qsend,
    qrecv,
    scores,
    q64,
    att64,
    att_all,
    wd_all,
    tok_all,
    po_send,
    po_recv,
    mixed,
    xs,
    row_send,
    row_recv,
    pd_send,
    pd_recv,
    hid,
    pe_send,
    pe_recv,
    er,
    er_recv,
    dense_part,
    fin_send,
    fin_recv,
    in_sem,
    local_sem,
    kv_sem,
    z_send,
    z_recv,
    j_send,
    j_recv,
    t_send,
    t_recv,
    ft_send,
    ft_recv,
    fm_send,
    fm_recv,
    p_send,
    p_recv,
):
    mz = lax.axis_index("z")
    mxx = lax.axis_index("x")
    mc = lax.axis_index("c")
    mt = lax.axis_index("tp")
    mj = mxx * NC + mc

    def zpeer(d):
        return lax.rem(mz + d, NZ)

    def zsource(d):
        return lax.rem(mz + NZ - d, NZ)

    def jpeer(d):
        return lax.rem(mj + d, NJ)

    def tpeer(d):
        return lax.rem(mt + d, NT)

    def zdev(d):
        return {"z": zpeer(d)}

    def jdev(d):
        j = jpeer(d)
        return {"x": lax.div(j, NC), "c": lax.rem(j, NC)}

    def away(k):
        x = lax.rem(mxx + k // 2, NX)
        c = lax.rem(mc + k % 2, NC)
        return x * NC + c, {"x": x, "c": c}

    def back_to(k):
        return {"x": lax.rem(mxx + NX - k // 2, NX), "c": lax.rem(mc + k % 2, NC)}

    def tdev(d):
        return {"tp": tpeer(d)}

    def remote(src, dst, ssem, rsem, dev):
        return pltpu.make_async_remote_copy(
            src_ref=src,
            dst_ref=dst,
            send_sem=ssem,
            recv_sem=rsem,
            device_id=dev,
            device_id_type=MESH_IDS,
        )

    started = []

    def exchange(order, make):
        copies = [make(d) for d in order]
        for copy in copies:
            copy.start()
        started.extend(copies)
        return copies

    def arrived(copies):
        for copy in reversed(copies):
            copy.wait_recv()

    barrier = pltpu.get_barrier_semaphore()
    for d in Z_ORDER:
        pl.semaphore_signal(barrier, inc=1, device_id=zdev(d), device_id_type=MESH_IDS)
    for d in J_ORDER:
        pl.semaphore_signal(barrier, inc=1, device_id=jdev(d), device_id_type=MESH_IDS)
    for d in T_ORDER:
        pl.semaphore_signal(barrier, inc=1, device_id=tdev(d), device_id_type=MESH_IDS)

    inputs = [
        pltpu.make_async_copy(src, dst, in_sem.at[k])
        for k, (src, dst) in enumerate(
            (
                (tokens_in, tokens),
                (attn_gain_in, attn_gain),
                (wq_hbm, wq_in),
                (wk_hbm, wk_in),
                (wv_hbm, wv_in),
                (route_ids_in, route_ids),
                (route_weights_in, route_weights),
                (wo_hbm, wo_in),
                (ffn_gain_in, ffn_gain),
                (branch_gate_in, branch_gate),
                (bias_hbm, bias),
                (lengths_hbm, lengths),
            )
        )
    ]
    for copy in inputs:
        copy.start()
    kv_copies = []
    for s in range(0, 16, 2):
        kv_copies.append(
            pltpu.make_async_copy(
                keys_hbm.at[pl.ds(s, 2), 0], keys.at[pl.ds(s, 2)], kv_sem.at[s]
            )
        )
    for s in range(0, 16, 2):
        kv_copies.append(
            pltpu.make_async_copy(
                values_hbm.at[pl.ds(s, 2), 0], values.at[pl.ds(s, 2)], kv_sem.at[s + 1]
            )
        )
    for copy in kv_copies:
        copy.start()
    dense_col = pl.ds(pl.multiple_of(mj * 128, 128), 128)
    locals_ = [
        pltpu.make_async_copy(dgate_hbm, dgate.at[:, dense_col], local_sem.at[0]),
        pltpu.make_async_copy(dup_hbm, dup.at[:, dense_col], local_sem.at[1]),
        pltpu.make_async_copy(ddown_hbm, ddown.at[dense_col], local_sem.at[2]),
        pltpu.make_async_copy(egate_hbm.at[0], egate, local_sem.at[3]),
        pltpu.make_async_copy(eup_hbm.at[0], eup, local_sem.at[4]),
        pltpu.make_async_copy(edown_hbm.at[0], edown, local_sem.at[5]),
    ]
    for copy in locals_:
        copy.start()

    for copy in inputs:
        copy.wait()

    pl.semaphore_wait(barrier, NJ + NZ + NT - 3)

    def chunk_of(src, dst, k, lo, hi):
        return exchange(
            J_ORDER,
            lambda d: remote(
                src.at[:, lo:hi],
                dst.at[mj, :, lo:hi],
                j_send.at[k, d],
                j_recv.at[k, d],
                jdev(d),
            ),
        )

    c_wa = chunk_of(wq_in, wq, 0, 0, 256)
    tok = tokens[...].astype(F32)
    normed = (
        tok * lax.rsqrt(jnp.mean(tok * tok, axis=-1, keepdims=True) + norm_eps) * attn_gain[...]
    ).astype(BF)
    for z in range(NZ):
        nsend[z] = normed[:, 256 * z : 256 * (z + 1)]
    c_n = exchange(
        Z_ORDER,
        lambda d: remote(
            nsend.at[zpeer(d)], nslab.at[mz], z_send.at[0, d], z_recv.at[0, d], zdev(d)
        ),
    )
    own_cols = pl.ds(pl.multiple_of(mt * 512, 512), 512)
    c_tok = exchange(
        Z_ORDER,
        lambda d: remote(
            tokens.at[:, own_cols],
            tok_all.at[mz, :, own_cols],
            z_send.at[4, d],
            z_recv.at[4, d],
            zdev(d),
        ),
    )
    c_wb = chunk_of(wq_in, wq, 1, 256, 512)
    c_wk = chunk_of(wk_in, wk, 2, 0, 128)
    c_wv = chunk_of(wv_in, wv, 9, 0, 128)
    c_wo = exchange(
        J_ORDER, lambda d: remote(wo_in, wo.at[mj], j_send.at[3, d], j_recv.at[3, d], jdev(d))
    )
    dense = (
        (dgate_hbm, lambda j: dgate.at[:, pl.ds(pl.multiple_of(j * 128, 128), 128)]),
        (dup_hbm, lambda j: dup.at[:, pl.ds(pl.multiple_of(j * 128, 128), 128)]),
        (ddown_hbm, lambda j: ddown.at[pl.ds(pl.multiple_of(j * 128, 128), 128)]),
    )
    c_dx = [
        exchange(
            (4, 2, 6),
            lambda d: remote(src, part(mj), j_send.at[4 + k, d], j_recv.at[4 + k, d], jdev(d)),
        )
        for k, (src, part) in enumerate(dense)
    ]
    partner = {"c": 1 - mc}
    c_dp = [
        exchange(
            (0,),
            lambda d: remote(src, part(mj), p_send.at[k, d], p_recv.at[k, d], partner),
        )
        for k, (src, part) in enumerate(dense)
    ]
    wq[mj] = wq_in[...]
    wk[mj] = wk_in[...]
    wv[mj] = wv_in[...]
    wo[mj] = wo_in[...]
    nslab[mz] = nsend[mz]
    tok_all[mz] = tokens[...]

    row_expert = lax.shift_right_logical(iota((128, 16), 0), 1)
    named = jnp.zeros((128, 16), F32)
    weighed = jnp.zeros((128, 16), F32)
    for k in range(4):
        hit = route_ids[k : k + 1, :] == row_expert
        named = named + one_if(hit)
        weighed = weighed + jnp.where(hit, route_weights[k : k + 1, :], 0.0)
    earlier = one_if(iota((16, 16), 0) < iota((16, 16), 1)).astype(BF)
    rank = dot(named.astype(BF), earlier)
    row_rank = jnp.bitwise_and(iota((128, 16), 0), 1).astype(F32)
    slots = jnp.where(rank == row_rank, weighed, 0.0)
    wd_all[mz] = jnp.concatenate([slots, jnp.zeros((128, 112), F32)], axis=1).T[0:16]

    def q_chunk(k, weight, lo, hi, at):
        width = hi - lo
        cols = slice(at, at + width)
        qsend[:, :, cols] = (
            dot(nslab[...].reshape(128, 256), weight[:, :, lo:hi].reshape(256, width))
            .astype(BF)
            .reshape(NZ, 16, width)
        )

    def q_exchange(k, lo, hi):
        copies = exchange(
            Z_ORDER,
            lambda d: remote(
                qsend.at[zpeer(d), :, lo:hi],
                qrecv.at[mz, :, lo:hi],
                z_send.at[k, d],
                z_recv.at[k, d],
                zdev(d),
            ),
        )
        qrecv[mz, :, lo:hi] = qsend[mz, :, lo:hi]
        return copies

    def q_sum(lo, hi):
        total = qrecv[0, :, lo:hi].astype(F32)
        for z in range(1, NZ):
            total = total + qrecv[z, :, lo:hi].astype(F32)
        return total.astype(BF)

    arrived(c_n)
    arrived(c_wa)
    q_chunk(0, wq, 0, 256, 0)
    c_qa = q_exchange(1, 0, 256)
    arrived(c_wb)
    q_chunk(1, wq, 256, 512, 256)
    c_qb = q_exchange(2, 256, 512)
    arrived(c_wk)
    arrived(c_wv)
    q_chunk(2, wk, 0, 128, 512)
    q_chunk(2, wv, 0, 128, 640)
    c_qc = q_exchange(3, 512, 768)
    c_wd = exchange(
        Z_ORDER,
        lambda d: remote(
            wd_all.at[mz], wd_all.at[mz], z_send.at[5, d], z_recv.at[5, d], zdev(d)
        ),
    )
    c_ftok = []
    for copy, d in reversed(list(zip(c_tok, Z_ORDER))):
        copy.wait_recv()
        block = tok_all.at[zsource(d), :, own_cols]
        c_ftok += exchange(
            T_ORDER,
            lambda e: remote(block, block, ft_send.at[d, e], ft_recv.at[d, e], tdev(e)),
        )

    for copy in kv_copies:
        copy.wait()
    arrived(c_qa)
    total_a = q_sum(0, 256)
    arrived(c_qb)
    total_b = q_sum(256, 512)

    q_rows = jnp.zeros((64, 128), F32)
    for h in range(4):
        part = (total_a, total_b)[h // 2][:, 128 * (h % 2) : 128 * (h % 2 + 1)]
        spread = one_if(iota((64, 16), 0) == 4 * iota((64, 16), 1) + h).astype(BF)
        q_rows = q_rows + dot(spread, part)
    q64[...] = q_rows
    first = iota((8, 128), 0) < 4
    for p in range(8):
        q8 = q64[8 * p : 8 * p + 8]
        qa = jnp.where(first, q8, 0.0).astype(BF)
        qb = jnp.where(first, 0.0, q8).astype(BF)
        scores[8 * p : 8 * p + 8] = dot_nt(qa, keys[2 * p]) + dot_nt(qb, keys[2 * p + 1])

    row = iota((64, 1), 0)
    head = jnp.bitwise_and(row, 3)
    seq = lax.shift_right_logical(row, 2)
    bias_col = jnp.zeros((64, 1), F32)
    for h in range(4):
        bias_col = jnp.where(head == h, bias[h], bias_col)
    len_col = jnp.zeros((64, 1), jnp.int32)
    for s in range(16):
        len_col = jnp.where(seq == s, lengths[s], len_col)
    after = one_if(iota((128, 128), 0) > iota((128, 128), 1)).astype(BF)
    carry = jnp.zeros((64, 1), F32)
    for b in reversed(range(8)):
        cols = slice(128 * b, 128 * (b + 1))
        zz = scores[:, cols] * (128 ** (-0.5)) + bias_col
        inside = (iota((64, 128), 1) + 128 * b) < len_col
        soft = jnp.log1p(jnp.exp(-jnp.abs(zz)))
        keep = jnp.where(inside, jnp.minimum(-zz, 0.0) - soft, 0.0)
        take = jnp.minimum(zz, 0.0) - soft
        k1 = keep.astype(BF)
        r1 = keep - k1.astype(F32)
        k2 = r1.astype(BF)
        k3 = (r1 - k2.astype(F32)).astype(BF)
        between = dot(k1, after) + dot(k2, after) + dot(k3, after) + carry
        carry = between[:, 0:1] + keep[:, 0:1]
        scores[:, cols] = jnp.where(inside, jnp.exp(take + between), 0.0)

    for p in range(8):
        w8 = scores[8 * p : 8 * p + 8].astype(BF)
        att64[8 * p : 8 * p + 8] = jnp.where(
            first, dot(w8, values[2 * p]), dot(w8, values[2 * p + 1])
        )
    att_rows = att64[...].astype(BF)
    for h in range(4):
        pick = one_if(iota((16, 64), 1) == 4 * iota((16, 64), 0) + h).astype(BF)
        att_all[mz, :, 128 * h : 128 * (h + 1)] = dot(pick, att_rows).astype(BF)

    c_a = exchange(
        Z_ORDER,
        lambda d: remote(
            att_all.at[mz], att_all.at[mz], z_send.at[6, d], z_recv.at[6, d], zdev(d)
        ),
    )
    arrived(c_qc)
    out[:, 512:768] = q_sum(512, 768)
    arrived(c_wd)
    slot_of_row = 16 * mz + 2 * lax.shift_right_logical(iota((128, 128), 0), 4)
    slot_of_row = slot_of_row + jnp.bitwise_and(iota((128, 128), 0), 1)
    spread = one_if(slot_of_row == iota((128, 128), 1)).astype(BF)
    row_z = jnp.bitwise_and(lax.shift_right_logical(iota((128, 128), 0), 1), 7)
    own_z = row_z == lax.shift_right_logical(iota((128, 128), 1), 4)
    wd = wd_all[...].reshape(128, 128)
    wd_hi = wd.astype(BF)
    wd_lo = (wd - wd_hi.astype(F32)).astype(BF)
    filled = one_if(wd > 0.0).astype(BF)
    dispatch = jnp.where(own_z, dot_nt(spread, filled), 0.0).astype(BF)
    row_z_t = jnp.bitwise_and(lax.shift_right_logical(iota((128, 128), 1), 1), 7)
    own_z_t = row_z_t == lax.shift_right_logical(iota((128, 128), 0), 4)
    comb_hi = jnp.where(own_z_t, dot_nt(wd_hi, spread), 0.0).astype(BF)
    comb_lo = jnp.where(own_z_t, dot_nt(wd_lo, spread), 0.0).astype(BF)
    arrived(c_wo)
    arrived(c_a)
    po_send[...] = (
        dot_nt(att_all[...].reshape(128, 512), wo[...].reshape(256, 512))
        .astype(BF)
        .reshape(NT, 32, 256)
    )
    c_po = exchange(
        T_ORDER,
        lambda d: remote(
            po_send.at[tpeer(d)], po_recv.at[mt], t_send.at[0, d], t_recv.at[0, d], tdev(d)
        ),
    )
    po_recv[mt] = po_send[mt]
    arrived(c_po)
    part = po_recv[0].astype(F32)
    for t in range(1, NT):
        part = part + po_recv[t].astype(F32)
    mixed[mt, mz] = part.astype(BF)

    own_block = mixed.at[mt, mz]
    c_mx = exchange(
        Z_ORDER,
        lambda d: remote(own_block, own_block, z_send.at[7, d], z_recv.at[7, d], zdev(d)),
    )
    c_fm = exchange(
        T_ORDER,
        lambda e: remote(own_block, own_block, fm_send.at[0, e], fm_recv.at[0, e], tdev(e)),
    )
    for copy, d in reversed(list(zip(c_mx, Z_ORDER))):
        copy.wait_recv()
        block = mixed.at[mt, zsource(d)]
        c_fm += exchange(
            T_ORDER,
            lambda e: remote(block, block, fm_send.at[d, e], fm_recv.at[d, e], tdev(e)),
        )
    for k, (src, part) in enumerate(dense):
        arrived(c_dx[k])
        c_dp[k] += exchange(
            (2, 4, 6),
            lambda d: remote(
                part(lax.rem(mj + NJ - d, NJ)),
                part(lax.rem(mj + NJ - d, NJ)),
                p_send.at[k, d // 2],
                p_recv.at[k, d // 2],
                partner,
            ),
        )
    for copy in c_ftok:
        copy.wait_recv()
    for copy in c_fm:
        copy.wait_recv()
    for z in range(NZ):
        pieces = []
        square = jnp.zeros((16, 1), F32)
        for s in range(NZ):
            cols = slice(256 * s, 256 * (s + 1))
            piece = tok_all[z, :, cols].astype(F32) + mixed[
                z // 2, s, 16 * (z % 2) : 16 * (z % 2) + 16
            ].astype(F32)
            square = square + jnp.sum(piece * piece, axis=-1, keepdims=True)
            pieces.append(piece)
        scale = lax.rsqrt(square * (1.0 / 2048) + norm_eps)
        for s in range(NZ):
            cols = slice(256 * s, 256 * (s + 1))
            xs[z, :, cols] = (pieces[s] * scale * ffn_gain[:, cols]).astype(BF)

    for copy in locals_:
        copy.wait()
    arrived(c_dp[0])
    arrived(c_dp[1])
    x_own = xs[:, :, own_cols].reshape(128, 512)
    c_pd = []
    for d in T_ORDER + (0,):
        to = tpeer(d)
        cols = pl.ds(pl.multiple_of(to * 256, 256), 256)
        block = pd_recv if d == 0 else pd_send
        block[to, :, 0:256] = dot(x_own, dgate[:, cols]).astype(BF)
        block[to, :, 256:512] = dot(x_own, dup[:, cols]).astype(BF)
        if d > 0:
            c_pd += exchange(
                (d,),
                lambda d: remote(
                    pd_send.at[to], pd_recv.at[mt], t_send.at[1, d], t_recv.at[1, d], tdev(d)
                ),
            )

    for b in range(4):
        cols = slice(512 * b, 512 * (b + 1))
        row_send[:, :, cols] = (
            dot(dispatch, xs[:, :, cols].reshape(128, 512)).astype(BF).reshape(NJ, 16, 512)
        )
    c_row = []
    for half, order in enumerate(((2, 6, 1), (4, 5, 3, 7))):
        c_row.append(
            exchange(
                order,
                lambda k: remote(
                    row_send.at[away(k)[0]],
                    row_recv.at[4 * half + HALVES[half].index(k)],
                    j_send.at[7, k],
                    j_recv.at[7, k],
                    away(k)[1],
                ),
            )
        )
    row_recv[0] = row_send[mj]

    weighted = jnp.zeros((128, 128), F32)
    for r in range(16):
        weighted = weighted + (
            xs[:, :, 128 * r : 128 * (r + 1)].reshape(128, 128).astype(F32)
            * branch_gate[r : r + 1, :].astype(F32)
        )
    branch = jax.nn.sigmoid(jnp.sum(weighted, axis=-1, keepdims=True))
    c_pe = []
    for half in range(2):
        arrived(c_row[half])
        rows = row_recv[4 * half : 4 * half + 4].reshape(64, 2048)
        gate_c = jnp.minimum(dot(rows, egate[...]), clamp_limit)
        up_c = jnp.clip(dot(rows, eup[...]), -clamp_limit, clamp_limit)
        unit = ((up_c + 1.0) * gate_c * jax.nn.sigmoid(swish_alpha * gate_c)).astype(BF)
        for t in range(NT):
            pe_send[half, t] = dot(unit, edown[:, 512 * t : 512 * (t + 1)]).astype(BF)
        c_pe.append(
            exchange(
                T_ORDER,
                lambda d: remote(
                    pe_send.at[half, tpeer(d)],
                    pe_recv.at[half, mt],
                    t_send.at[3 + half, d],
                    t_recv.at[3 + half, d],
                    tdev(d),
                ),
            )
        )
        pe_recv[half, mt] = pe_send[half, mt]

    arrived(c_pd)
    pre = pd_recv[0].astype(F32)
    for t in range(1, NT):
        pre = pre + pd_recv[t].astype(F32)
    gate_d = pre[:, 0:256]
    hid[mt] = (gate_d * jax.nn.sigmoid(gate_d) * pre[:, 256:512]).astype(BF)
    c_h = exchange(
        T_ORDER,
        lambda d: remote(hid.at[mt], hid.at[mt], t_send.at[2, d], t_recv.at[2, d], tdev(d)),
    )

    c_er = []
    for half in range(2):
        arrived(c_pe[half])
        total_e = pe_recv[half, 0].astype(F32)
        for t in range(1, NT):
            total_e = total_e + pe_recv[half, t].astype(F32)
        er[4 * half : 4 * half + 4] = total_e.astype(BF).reshape(4, 16, 512)
        c_er += exchange(
            ((2, 6, 1), (4, 5, 3, 7))[half],
            lambda k: remote(
                er.at[4 * half + HALVES[half].index(k)],
                er_recv.at[mj],
                j_send.at[8, k],
                j_recv.at[8, k],
                back_to(k),
            ),
        )
    er_recv[mj] = er[0]

    arrived(c_h)
    arrived(c_dp[2])
    down = dot(hid[0], ddown[0:256])
    for t in range(1, NT):
        down = down + dot(hid[t], ddown[256 * t : 256 * (t + 1)])
    dense_part[...] = down * branch

    arrived(c_er)
    back = er_recv[...].reshape(128, 512)
    fin_send[...] = (
        (dot(comb_hi, back) + dot(comb_lo, back) + dense_part[...]).astype(BF).reshape(NZ, 16, 512)
    )
    c_f = exchange(
        Z_ORDER,
        lambda d: remote(
            fin_send.at[zpeer(d)], fin_recv.at[mz], z_send.at[8, d], z_recv.at[8, d], zdev(d)
        ),
    )
    fin_recv[mz] = fin_send[mz]
    quarter = lax.div(mz, 2)
    own_rows = pl.ds(pl.multiple_of(lax.rem(mz, 2) * 16, 16), 16)
    final = tokens[:, own_cols].astype(F32) + jnp.concatenate(
        [mixed[quarter, 2 * mt, own_rows], mixed[quarter, 2 * mt + 1, own_rows]], axis=1
    ).astype(F32)
    arrived(c_f)
    for z in range(NZ):
        final = final + fin_recv[z].astype(F32)
    out[:, 0:512] = final.astype(BF)

    for copy in started:
        copy.wait_send()


def split_kernel(both, layer_out, new_keys, new_values):
    layer_out[...] = both[:, 0:512]
    new_keys[...] = both[:, 512:640]
    new_values[...] = both[:, 640:768]


def body(
    tokens,
    attn_gain,
    query_weight,
    key_weight,
    value_weight,
    break_bias,
    cache_keys,
    cache_values,
    lengths,
    out_weight,
    ffn_gain,
    branch_gate,
    dense_gate,
    dense_up,
    dense_down,
    route_ids,
    route_weights,
    expert_gate,
    expert_up,
    expert_down,
):
    vm = pl.BlockSpec(memory_space=pltpu.VMEM)
    hbm = pl.BlockSpec(memory_space=pl.ANY)
    V = pltpu.VMEM
    D = pltpu.SemaphoreType.DMA
    both = pl.pallas_call(
        kernel,
        name="layer",
        out_shape=jax.ShapeDtypeStruct((16, 768), BF),
        in_specs=[hbm] * 20,
        out_specs=vm,
        scratch_shapes=[
            V((16, 2048), BF),
            V((1, 2048), F32),
            V((32, 512), BF),
            V((32, 128), BF),
            V((32, 128), BF),
            V((32, 512), BF),
            V((1, 2048), F32),
            V((16, 128), BF),
            V((4, 16), jnp.int32),
            V((4, 16), F32),
            pltpu.SMEM((4,), F32),
            pltpu.SMEM((16,), jnp.int32),
            V((16, 1024, 128), BF),
            V((16, 1024, 128), BF),
            V((2048, 256), BF),
            V((2048, 256), BF),
            V((256, 2048), BF),
            V((512, 1024), BF),
            V((512, 1024), BF),
            V((1024, 512), BF),
            V((NJ, 32, 512), BF),
            V((NJ, 32, 128), BF),
            V((NJ, 32, 128), BF),
            V((NJ, 32, 512), BF),
            V((NZ, 16, 256), BF),
            V((NZ, 16, 256), BF),
            V((NZ, 16, 768), BF),
            V((NZ, 16, 768), BF),
            V((64, 1024), F32),
            V((64, 128), F32),
            V((64, 128), F32),
            V((NZ, 16, 512), BF),
            V((NZ, 16, 128), F32),
            V((NZ, 16, 2048), BF),
            V((NT, 32, 256), BF),
            V((NT, 32, 256), BF),
            V((NT, NZ, 32, 256), BF),
            V((NZ, 16, 2048), BF),
            V((NJ, 16, 2048), BF),
            V((NJ, 16, 2048), BF),
            V((NT, 128, 512), BF),
            V((NT, 128, 512), BF),
            V((NT, 128, 256), BF),
            V((2, NT, 64, 512), BF),
            V((2, NT, 64, 512), BF),
            V((NJ, 16, 512), BF),
            V((NJ, 16, 512), BF),
            V((128, 512), F32),
            V((NZ, 16, 512), BF),
            V((NZ, 16, 512), BF),
            D((12,)),
            D((6,)),
            D((16,)),
            D((9, NZ)),
            D((9, NZ)),
            D((10, NJ)),
            D((10, NJ)),
            D((5, NT)),
            D((5, NT)),
            D((NZ, NT)),
            D((NZ, NT)),
            D((NZ, NT)),
            D((NZ, NT)),
            D((3, 4)),
            D((3, 4)),
        ],
        compiler_params=pltpu.CompilerParams(
            collective_id=0,
            has_side_effects=True,
            vmem_limit_bytes=60 * 1024 * 1024,
        ),
    )(
        tokens,
        attn_gain.reshape(1, -1),
        query_weight,
        key_weight,
        value_weight,
        break_bias,
        cache_keys,
        cache_values,
        lengths,
        out_weight.T,
        ffn_gain.reshape(1, -1),
        branch_gate.reshape(16, 128),
        dense_gate,
        dense_up,
        dense_down,
        route_ids.T,
        route_weights.T,
        expert_gate,
        expert_up,
        expert_down,
    )
    return tuple(
        pl.pallas_call(
            split_kernel,
            name="split",
            out_shape=(
                jax.ShapeDtypeStruct((16, 512), BF),
                jax.ShapeDtypeStruct((16, 128), BF),
                jax.ShapeDtypeStruct((16, 128), BF),
            ),
            in_specs=[vm],
            out_specs=(vm, vm, vm),
        )(both)
    )


def solution(mesh):
    split = Mesh(mesh.devices.reshape(NZ, NX, NC, NT), ("z", "x", "c", "tp"))
    return jax.shard_map(
        body,
        mesh=split,
        in_specs=(
            P(EP, None),
            P(),
            P(EP, "tp"),
            P(EP, "tp"),
            P(EP, "tp"),
            P("tp"),
            P(EP, "tp", None, None),
            P(EP, "tp", None, None),
            P(EP),
            P("tp", EP),
            P(),
            P(),
            P("tp", EP),
            P("tp", EP),
            P(EP, "tp"),
            P(EP, None),
            P(EP, None),
            P(EP, None, "tp"),
            P(EP, None, "tp"),
            P(EP, "tp", None),
        ),
        out_specs=(P(EP, "tp"), P(EP, "tp"), P(EP, "tp")),
        check_vma=False,
    )
```
